256 devices in a mesh: sp: 32 (over z, x), tp: 8 (over y, core).
Axes of the slice: x: 4, y: 4, z: 8, core: 2. Of those that a mesh axis runs over, the one named last changes fastest.
Arguments:
- queries: bfloat16 [24576, 2048], P('sp', 'tp'), may hold values from -110 to 110
- key_rows: bfloat16 [24576, 512], P('sp', 'tp'), may hold values from -4.5 to 4.5
- values: bfloat16 [24576, 512], P('sp', 'tp'), may hold values from -6 to 6
- sink_logits: float32 [32], P('tp'), may hold values from 2 to 7
- doc_ids: int32 [24576], P('sp'), may hold values from 0 to 15, as said below
- residual: bfloat16 [24576, 2048], P('sp'), may hold values from -20 to 20
- w_out: bfloat16 [2048, 2048], P('tp'), may hold values from -2.390625 to 2.390625
- norm_gain: float32 [2048], replicated, may hold values from 0.1 to 1.9
- w_value_up: bfloat16 [2048, 5632], P('sp', 'tp'), may hold values from -0.125 to 0.125
- w_gate_up: bfloat16 [2048, 5632], P('sp', 'tp'), may hold values from -0.125 to 0.125
- conv_taps: bfloat16 [3, 5632], P(None, 'tp'), may hold values from -3.5 to 3.5
- w_down_t: bfloat16 [2048, 5632], P('sp', 'tp'), may hold values from -0.078125 to 0.078125
Outputs:
- layer_out: bfloat16 [24576, 2048], P('sp', 'tp')
The draws below stay inside these ranges and needn't reach their ends.
Inputs may be any that keep to these rules, and one draw needn't show every extreme that they name: `doc_ids`: document numbers never fall along the sequence and every one of the 16 documents is present; each document has 2 or more positions.
All inputs are finite; a program needn't handle non-finite values.
Results may differ from the reference program's by a relative error of at most 0.017.
Values may be sent and summed in bfloat16 or wider, within the bound.
No kernel may reach another device: no remote copies, remote signals or barrier semaphores. Data moves between devices by JAX's collectives and lax.ppermute only.
A program may use at most 64 MiB of HBM per device.

```python
import jax
import jax.numpy as jnp
from jax import lax

D = 2048
FF = 5632
HEADS = 32
KV_HEADS = 8
HEAD_DIM = 64
WINDOW = 128
TOK_DEV = 768
Q_W = 2048
SEQ = 24576
DOCS = 16
N_TP = 8


def paired_heads(key):
    key_part = jnp.clip(jax.random.normal(jax.random.fold_in(key, 11), (SEQ, KV_HEADS, HEAD_DIM), jnp.float32), -4.0, 4.0)
    query_part = jnp.clip(jax.random.normal(jax.random.fold_in(key, 12), (SEQ, HEADS, HEAD_DIM), jnp.float32), -5.0, 5.0)
    return (query_part.reshape(SEQ, HEADS * HEAD_DIM), key_part.reshape(SEQ, KV_HEADS * HEAD_DIM))


def draw_queries(key, part):
    return paired_heads(key)[0].astype(jnp.bfloat16)


def draw_key_rows(key, part):
    return paired_heads(key)[1].astype(jnp.bfloat16)


def draw_doc_ids(key, part):
    starts_count = DOCS - 1
    centre = 2 * TOK_DEV * (jnp.arange(starts_count, dtype=jnp.int32) + 1)
    offset = jax.random.randint(jax.random.fold_in(key, 31), (starts_count,), 1 - TOK_DEV, TOK_DEV, jnp.int32)
    starts = centre + offset
    position = jnp.arange(SEQ, dtype=jnp.int32)
    return jnp.sum((position[:, None] >= starts[None, :]).astype(jnp.int32), axis=1).astype(jnp.int32)


def draw_residual(key, part):
    column = jnp.arange(D).astype(jnp.float32)
    col_scale = 0.5 * jnp.exp(jnp.log(3.0) * column / (D - 1))
    draws_base = jnp.clip(jax.random.normal(jax.random.fold_in(key, 21), (SEQ, D), jnp.float32), -4.0, 4.0)
    return (draws_base * col_scale[None, :]).astype(jnp.bfloat16)


def level_of(rng, dims, shards, smallest, high):
    loudness, own = 1.0, jax.random.fold_in(rng, 6)
    for dim, blocks in shards:
        draws = jnp.exp(jax.random.uniform(jax.random.fold_in(own, dim), (blocks,), jnp.float32, smallest / len(shards), high / len(shards)))
        loudness = loudness * jnp.repeat(draws, dims[dim] // blocks).reshape([-1 if axis == dim else 1 for axis in range(len(dims))])
    return loudness


def scatter_about(stream_key, extent, deviation, most, split=(), held_as=jnp.bfloat16):
    values = jax.random.normal(stream_key, extent, jnp.float32) * deviation
    if len(split) > 0:
        values = level_of(stream_key, extent, split, -0.22, 0.18) * values
    return jnp.clip(values, min=-most, max=most).astype(held_as)


def setup_inputs(seed: int = 0) -> dict:
    key_of = jax.random.split(jax.random.key(seed), 13)
    return {
        "queries": draw_queries(jax.random.fold_in(key_of[12], 71), 0),
        "key_rows": draw_key_rows(jax.random.fold_in(key_of[12], 71), 0),
        "values": scatter_about(key_of[2], (SEQ, KV_HEADS * HEAD_DIM), 1.0, 6.0, ((0, 32), (1, 8))),
        "sink_logits": jnp.clip(2.0 + 5.0 * jax.random.uniform(key_of[3], (HEADS,), jnp.float32) ** level_of(key_of[3], (HEADS,), ((0, 8),), -0.2, 0.2), 2.0, 7.0),
        "doc_ids": draw_doc_ids(jax.random.fold_in(key_of[12], 71), 0),
        "residual": draw_residual(jax.random.fold_in(key_of[12], 71), 0),
        "w_out": scatter_about(key_of[6], (Q_W, D), 0.4, 2.390625, ((0, 8),)),
        "norm_gain": jnp.clip(1.0 + 0.18 * jax.random.normal(key_of[7], (D,), jnp.float32), 0.1, 1.9),
        "w_value_up": scatter_about(key_of[8], (D, FF), D ** -0.5, 0.125, ((0, 32), (1, 8))),
        "w_gate_up": scatter_about(key_of[9], (D, FF), D ** -0.5, 0.125, ((0, 32), (1, 8))),
        "conv_taps": scatter_about(key_of[10], (3, FF), 3 ** -0.5, 3.5, ((1, 8),)),
        "w_down_t": scatter_about(key_of[11], (D, FF), FF ** -0.5, 0.078125, ((0, 32), (1, 8))),
    }


EPS = 1e-06
NEG = -1e+30

def attend_block(q_block, kv_window, doc_window, doc_query, sink_logits):
    per_kv = HEADS // KV_HEADS
    kv_cols = KV_HEADS * HEAD_DIM
    q_heads = q_block.astype(jnp.float32).reshape(WINDOW, KV_HEADS, per_kv, HEAD_DIM)
    k_heads = kv_window[:, :kv_cols].astype(jnp.float32).reshape(3 * WINDOW, KV_HEADS, HEAD_DIM)
    v_heads = kv_window[:, kv_cols:].astype(jnp.float32).reshape(3 * WINDOW, KV_HEADS, HEAD_DIM)
    score = jnp.einsum('qkgd,jkd->kgqj', q_heads, k_heads) * HEAD_DIM ** (-0.5)
    offsets = jnp.arange(3 * WINDOW)[None, :] - WINDOW - jnp.arange(WINDOW)[:, None]
    allowed = (jnp.abs(offsets) <= WINDOW) & (doc_query[:, None] == doc_window[None, :])
    sink_grid = sink_logits.reshape(KV_HEADS, per_kv)[:, :, None]
    highest = jnp.maximum(lax.optimization_barrier(jnp.max(jnp.where(allowed, score, NEG), axis=-1)), sink_grid)
    raw = jnp.where(allowed, jnp.exp(score - highest[..., None]), 0.0)
    total = lax.optimization_barrier(jnp.sum(raw, axis=-1)) + jnp.exp(sink_grid - highest)
    probs = (raw / total[..., None]).astype(jnp.bfloat16)
    attended = jnp.einsum('kgqj,jkd->qkgd', probs.astype(jnp.float32), v_heads)
    return attended.reshape(WINDOW, HEADS * HEAD_DIM).astype(jnp.bfloat16)

def rounded(term):
    return lax.optimization_barrier(term.astype(jnp.bfloat16)).astype(jnp.float32)

def reference(queries, key_rows, values, sink_logits, doc_ids, residual, w_out, norm_gain, w_value_up, w_gate_up, conv_taps, w_down_t):
    seq_len = queries.shape[0]
    blocks = seq_len // WINDOW
    stacked = jnp.concatenate([key_rows, values], axis=1)
    padded = jnp.pad(stacked, ((WINDOW, WINDOW), (0, 0)))
    labels = doc_ids + 1
    label_pad = jnp.pad(labels, (WINDOW, WINDOW))
    kv_blocks = padded.reshape(blocks + 2, WINDOW, stacked.shape[1])
    kv_window = jnp.concatenate([kv_blocks[:-2], kv_blocks[1:-1], kv_blocks[2:]], axis=1)
    lab_blocks = label_pad.reshape(blocks + 2, WINDOW)
    doc_window = jnp.concatenate([lab_blocks[:-2], lab_blocks[1:-1], lab_blocks[2:]], axis=1)
    q_blocks = queries.reshape(blocks, WINDOW, queries.shape[1])
    doc_query = labels.reshape(blocks, WINDOW)
    attended = lax.map(lambda items: attend_block(items[0], items[1], items[2], items[3], sink_logits), (q_blocks, kv_window, doc_window, doc_query))
    attended = attended.reshape(seq_len, queries.shape[1])
    head_cols = queries.shape[1] // N_TP
    attn_total = jnp.zeros((seq_len, D), jnp.float32)
    for member in range(N_TP):
        cols = attended[:, member * head_cols:(member + 1) * head_cols]
        rows_w = w_out[member * head_cols:(member + 1) * head_cols]
        attn_total = attn_total + rounded(jnp.dot(cols, rows_w, preferred_element_type=jnp.float32))
    mixed = (residual.astype(jnp.float32) + attn_total).astype(jnp.bfloat16)
    mixed_f = mixed.astype(jnp.float32)
    mean_sq = lax.optimization_barrier(jnp.mean(mixed_f * mixed_f, axis=1, keepdims=True))
    normed = (mixed_f * lax.rsqrt(mean_sq + EPS) * norm_gain).astype(jnp.bfloat16)
    up_value = jnp.dot(normed, w_value_up, preferred_element_type=jnp.float32).astype(jnp.bfloat16)
    up_gate = jnp.dot(normed, w_gate_up, preferred_element_type=jnp.float32).astype(jnp.bfloat16)
    value_f = up_value.astype(jnp.float32)
    value_pad = jnp.pad(value_f, ((1, 1), (0, 0)))
    lab_one = jnp.pad(labels, (1, 1))
    prev_same = (lab_one[:-2] == labels)[:, None]
    next_same = (lab_one[2:] == labels)[:, None]
    tap_f = conv_taps.astype(jnp.float32)
    conv = tap_f[0] * jnp.where(prev_same, value_pad[:-2], 0.0) + tap_f[1] * value_f + tap_f[2] * jnp.where(next_same, value_pad[2:], 0.0)
    hidden = (jax.nn.silu(conv) * up_gate.astype(jnp.float32)).astype(jnp.bfloat16)
    ff_cols = FF // N_TP
    ffn_total = jnp.zeros((seq_len, D), jnp.float32)
    for member in range(N_TP):
        cols = hidden[:, member * ff_cols:(member + 1) * ff_cols]
        down_cols = w_down_t[:, member * ff_cols:(member + 1) * ff_cols]
        term = lax.dot_general(cols, down_cols, (((1,), (1,)), ((), ())), preferred_element_type=jnp.float32)
        ffn_total = ffn_total + rounded(term)
    return (mixed.astype(jnp.float32) + ffn_total).astype(jnp.bfloat16)
```

```python
import jax
import jax.numpy as jnp
from jax import lax
from jax.sharding import PartitionSpec as P

HEAD_DIM = 64
WINDOW = 128
EPS = 1e-06
NEG = -1e30

NZ, NX, NY, NC = 8, 4, 4, 2


def sp_shift(dz, dx):
    return [
        (z * NX + x, ((z + dz) % NZ) * NX + (x + dx) % NX) for z in range(NZ) for x in range(NX)
    ]


def tp_shift(dy, dc):
    return [
        (y * NC + c, ((y + dy) % NY) * NC + (c + dc) % NC) for y in range(NY) for c in range(NC)
    ]


def put(block, piece, at):
    start = [at] + [0] * (block.ndim - 1)
    return lax.dynamic_update_slice(block, piece[None], start)


def gather_x(own, x, shape_tail):
    out = jnp.zeros((NX,) + own.shape, own.dtype)
    out = put(out, own, x)
    for k in range(1, NX):
        got = lax.ppermute(own, "sp", sp_shift(0, k))
        out = put(out, got, (x - k) % NX)
    return out


def gather_z(own, z):
    out = jnp.zeros((NZ,) + own.shape, own.dtype)
    out = put(out, own, z)
    up, down = own, own
    for k in range(1, NZ // 2):
        up = lax.ppermute(up, "sp", sp_shift(1, 0))
        down = lax.ppermute(down, "sp", sp_shift(-1, 0))
        out = put(out, up, (z - k) % NZ)
        out = put(out, down, (z + k) % NZ)
    half = own.shape[0] // 2
    last = jnp.concatenate(
        [
            lax.ppermute(up[:half], "sp", sp_shift(1, 0)),
            lax.ppermute(down[half:], "sp", sp_shift(-1, 0)),
        ],
        axis=0,
    )
    return put(out, last, (z + NZ // 2) % NZ)


def extended(block, width):
    count = lax.axis_size("sp")
    forward = [(i, i + 1) for i in range(count - 1)]
    backward = [(target, source) for source, target in forward]
    low = lax.ppermute(block[-width:], "sp", forward)
    high = lax.ppermute(block[:width], "sp", backward)
    return jnp.concatenate([low, block, high], axis=0)


def local_attention(queries, rim_kv, rim_labels, labels, sink_logits, kv_cols):
    rows_here = queries.shape[0]
    blocks = rows_here // WINDOW
    kv_local = kv_cols // HEAD_DIM
    heads_here = queries.shape[1] // HEAD_DIM
    per_kv = heads_here // kv_local
    kv_blocks = rim_kv.reshape(blocks + 2, WINDOW, rim_kv.shape[1])
    kv_window = jnp.concatenate([kv_blocks[:-2], kv_blocks[1:-1], kv_blocks[2:]], axis=1)
    lab_blocks = rim_labels.reshape(blocks + 2, WINDOW)
    doc_window = jnp.concatenate([lab_blocks[:-2], lab_blocks[1:-1], lab_blocks[2:]], axis=1)
    q_blocks = queries.reshape(blocks, WINDOW, kv_local, per_kv, HEAD_DIM)
    k_blocks = kv_window[:, :, :kv_cols].reshape(blocks, 3 * WINDOW, kv_local, HEAD_DIM)
    v_blocks = kv_window[:, :, kv_cols:].reshape(blocks, 3 * WINDOW, kv_local, HEAD_DIM)
    score = jnp.einsum(
        "nqkgd,njkd->nkgqj", q_blocks, k_blocks, preferred_element_type=jnp.float32
    ) * HEAD_DIM ** (-0.5)
    offsets = jnp.arange(3 * WINDOW)[None, :] - WINDOW - jnp.arange(WINDOW)[:, None]
    in_band = jnp.abs(offsets) <= WINDOW
    doc_query = labels.reshape(blocks, WINDOW)
    allowed = in_band[None] & (doc_query[:, :, None] == doc_window[:, None, :])
    allowed = allowed[:, None, None, :, :]
    sink_grid = sink_logits.reshape(kv_local, per_kv)[None, :, :, None]
    highest = jnp.maximum(jnp.max(jnp.where(allowed, score, NEG), axis=-1), sink_grid)
    raw = jnp.where(allowed, jnp.exp(score - highest[..., None]), 0.0)
    total = jnp.sum(raw, axis=-1) + jnp.exp(sink_grid - highest)
    probs = (raw / total[..., None]).astype(jnp.bfloat16)
    attended = jnp.einsum("nkgqj,njkd->nqkgd", probs, v_blocks, preferred_element_type=jnp.float32)
    return attended.reshape(rows_here, queries.shape[1]).astype(jnp.bfloat16)


def scattered_sum(mine, theirs):
    got = lax.ppermute(theirs, "tp", tp_shift(0, 1))
    span = got.shape[1] // NY
    pair = (mine + got.astype(jnp.float32)).astype(jnp.bfloat16)
    total = pair[:, :span].astype(jnp.float32)
    for k in range(1, NY):
        block = pair[:, k * span : (k + 1) * span]
        total = total + lax.ppermute(block, "tp", tp_shift(k, 0)).astype(jnp.float32)
    return total


def per_device(
    queries,
    key_rows,
    values,
    sink_logits,
    doc_ids,
    residual,
    w_out,
    norm_gain,
    w_value_up,
    w_gate_up,
    conv_taps,
    w_down_t,
):
    rows_here = queries.shape[0]
    model_width = residual.shape[1]
    span = model_width // (NY * NC)
    ff = w_value_up.shape[1]
    sp, tp = lax.axis_index("sp"), lax.axis_index("tp")
    z, x, y, core = sp // NX, sp % NX, tp // NC, tp % NC

    tail = ff - ff % 128
    share_a = jnp.concatenate([w_value_up, w_gate_up[:, tail:], w_gate_up[:, :384]], axis=1)
    share_b = jnp.concatenate([w_gate_up[:, 384:tail], w_down_t], axis=1)
    rows_w = share_a.shape[0]
    block_a = gather_x(share_a, x, None).reshape(NX * rows_w, -1)
    full_a = gather_z(block_a, z).reshape(model_width, -1)
    block_b = gather_z(share_b, z)
    full_b = jnp.swapaxes(gather_x(block_b, x, None), 0, 1).reshape(model_width, -1)

    kv_cols = key_rows.shape[1]
    stacked = jnp.concatenate([key_rows, values], axis=1)
    labels = doc_ids + 1
    rim_kv = extended(stacked, WINDOW)
    rim_labels = extended(labels, WINDOW)
    attended = local_attention(queries, rim_kv, rim_labels, labels, sink_logits, kv_cols)

    def cols_of(w, who, axis):
        return jnp.concatenate(
            [
                lax.dynamic_slice_in_dim(w, (((y + k) % NY) * NC + who) * span, span, axis)
                for k in range(NY)
            ],
            axis=axis,
        )

    theirs = jnp.dot(attended, cols_of(w_out, 1 - core, 1), preferred_element_type=jnp.float32)
    mine = jnp.dot(attended, cols_of(w_out, core, 1), preferred_element_type=jnp.float32)
    summed = scattered_sum(mine, theirs.astype(jnp.bfloat16))
    own_res = lax.dynamic_slice_in_dim(residual, tp * span, span, 1)
    mixed_own = (own_res.astype(jnp.float32) + summed).astype(jnp.bfloat16)

    parts = [mixed_own] + [lax.ppermute(mixed_own, "tp", tp_shift(k, 0)) for k in range(1, NY)]
    own4 = jnp.concatenate(parts, axis=1)
    got4 = lax.ppermute(own4, "tp", tp_shift(0, 1))
    mixed = jnp.zeros((rows_here, model_width), jnp.bfloat16)
    for k in range(NY):
        at = ((y - k) % NY) * NC
        mixed = lax.dynamic_update_slice(mixed, parts[k], (0, (at + core) * span))
        mixed = lax.dynamic_update_slice(
            mixed, got4[:, k * span : (k + 1) * span], (0, (at + 1 - core) * span)
        )
    mixed_f = mixed.astype(jnp.float32)
    mean_sq = jnp.mean(mixed_f * mixed_f, axis=1, keepdims=True)
    normed = (mixed_f * lax.rsqrt(mean_sq + EPS) * norm_gain).astype(jnp.bfloat16)

    up_a = jnp.dot(normed, full_a, preferred_element_type=jnp.float32).astype(jnp.bfloat16)
    up_b = jnp.dot(normed, full_b[:, : tail - 384], preferred_element_type=jnp.float32).astype(
        jnp.bfloat16
    )
    full_down = full_b[:, tail - 384 :]
    up_value = up_a[:, :ff]
    up_gate = jnp.concatenate([up_a[:, ff + ff - tail :], up_b, up_a[:, ff : ff + ff - tail]], axis=1)
    rim_value = extended(up_value, 1).astype(jnp.float32)
    prev_same = (rim_labels[WINDOW - 1 : WINDOW - 1 + rows_here] == labels)[:, None]
    next_same = (rim_labels[WINDOW + 1 : WINDOW + 1 + rows_here] == labels)[:, None]
    tap_f = conv_taps.astype(jnp.float32)
    conv = (
        tap_f[0] * jnp.where(prev_same, rim_value[:-2], 0.0)
        + tap_f[1] * up_value.astype(jnp.float32)
        + tap_f[2] * jnp.where(next_same, rim_value[2:], 0.0)
    )
    hidden = (jax.nn.silu(conv) * up_gate.astype(jnp.float32)).astype(jnp.bfloat16)

    def down(who):
        return lax.dot_general(
            hidden,
            cols_of(full_down, who, 0),
            (((1,), (1,)), ((), ())),
            preferred_element_type=jnp.float32,
        )

    ffn_cols = scattered_sum(down(core), down(1 - core).astype(jnp.bfloat16))
    return (mixed_own.astype(jnp.float32) + ffn_cols).astype(jnp.bfloat16)


def solution(mesh):
    placed = (
        P("sp", "tp"),
        P("sp", "tp"),
        P("sp", "tp"),
        P("tp"),
        P("sp"),
        P("sp", None),
        P("tp", None),
        P(),
        P("sp", "tp"),
        P("sp", "tp"),
        P(None, "tp"),
        P("sp", "tp"),
    )
    return jax.shard_map(
        per_device, mesh=mesh, in_specs=placed, out_specs=P("sp", "tp"), check_vma=False
    )
```

```python
import functools

import jax
import jax.numpy as jnp
from jax import lax
from jax.experimental import pallas as pl
from jax.experimental.pallas import tpu as pltpu
from jax.sharding import PartitionSpec as P

HEAD_DIM = 64
WINDOW = 128
EPS = 1e-06
NEG = -1e30

NZ, NX, NY, NC = 8, 4, 4, 2
MB = 1 << 20


def tp_shift(dy, dc):
    return [
        (y * NC + c, ((y + dy) % NY) * NC + (c + dc) % NC) for y in range(NY) for c in range(NC)
    ]


def index_of(z, x, y, c):
    return (((z % NZ) * NX + x % NX) * NY + y % NY) * NC + c


def apart(dz, dx):
    return [
        (index_of(z, x, y, c), index_of(z + s * dz, x + s * dx, y, c))
        for z in range(NZ)
        for x in range(NX)
        for y in range(NY)
        for c, s in ((0, 1), (1, -1))
    ]


def send_apart(block, dz, dx):
    return lax.ppermute(block, ("sp", "tp"), apart(dz, dx))


def swap(block):
    return lax.ppermute(block, "tp", tp_shift(0, 1))


def after(value, *others):
    return lax.optimization_barrier((value,) + others)[0]


def pick(block, at):
    return lax.dynamic_index_in_dim(block, at, 0, keepdims=False)


def put(block, piece, *at):
    piece = piece.reshape((1,) * (block.ndim - piece.ndim) + piece.shape)
    start = list(at) + [0] * (block.ndim - len(at))
    return lax.dynamic_update_slice(block, piece, start)


def attention_kernel(
    at_ref, sink_ref, q_ref, kt_ref, vt_ref, lab_ref, low_ref, high_ref, w_ref,
    att_ref, t0_ref, t1_ref, t2_ref, t3_ref, kx_ref, vx_ref, row_ref, col_ref,
):
    rows = q_ref.shape[0]
    heads = q_ref.shape[1] // HEAD_DIM
    span = t0_ref.shape[1]
    kx_ref[...] = jnp.zeros_like(kx_ref)
    vx_ref[...] = jnp.zeros_like(vx_ref)
    pieces = (
        (0, WINDOW, low_ref[:HEAD_DIM], low_ref[HEAD_DIM : 2 * HEAD_DIM]),
        (WINDOW, rows, kt_ref[...], vt_ref[...]),
        (WINDOW + rows, WINDOW, high_ref[:HEAD_DIM], high_ref[HEAD_DIM : 2 * HEAD_DIM]),
    )
    for start, width, keys, vals in pieces:
        vals_t = vals.astype(jnp.float32).T.astype(jnp.bfloat16)
        for h in range(heads):
            kx_ref[h, h * HEAD_DIM : (h + 1) * HEAD_DIM, start : start + width] = keys
            vx_ref[h, start : start + width, h * HEAD_DIM : (h + 1) * HEAD_DIM] = vals_t
    row_ref[:, :WINDOW] = jnp.broadcast_to(
        low_ref[2 * HEAD_DIM :].astype(jnp.float32), (8, WINDOW)
    )
    row_ref[:, WINDOW : WINDOW + rows] = jnp.broadcast_to(lab_ref[...], (8, rows))
    row_ref[:, WINDOW + rows :] = jnp.broadcast_to(
        high_ref[2 * HEAD_DIM :].astype(jnp.float32), (8, WINDOW)
    )
    for n in range(rows // WINDOW):
        part = row_ref[:, (n + 1) * WINDOW : (n + 2) * WINDOW]
        col_ref[n * WINDOW : (n + 1) * WINDOW, :] = jnp.broadcast_to(
            part[:1], (WINDOW, WINDOW)
        ).T

    def step(n, carry):
        base = pl.multiple_of(n * WINDOW, WINDOW)
        here = pl.ds(base, WINDOW)
        window = pl.ds(base, 3 * WINDOW)
        q = q_ref[here, :] * jnp.bfloat16(HEAD_DIM ** (-0.5))
        offsets = (
            lax.broadcasted_iota(jnp.int32, (WINDOW, 3 * WINDOW), 1)
            - WINDOW
            - lax.broadcasted_iota(jnp.int32, (WINDOW, 3 * WINDOW), 0)
        )
        mine = col_ref[here, :1]
        allowed = (jnp.abs(offsets) <= WINDOW) & (row_ref[:1, window] == mine)
        acc = None
        for h in range(heads):
            score = jnp.dot(q, kx_ref[h, :, window], preferred_element_type=jnp.float32)
            score = jnp.where(allowed, score, NEG)
            highest = jnp.maximum(jnp.max(score, axis=1, keepdims=True), sink_ref[h])
            raw = jnp.exp(score - highest)
            total = jnp.sum(raw, axis=1, keepdims=True) + jnp.exp(sink_ref[h] - highest)
            probs = (raw * (1.0 / total)).astype(jnp.bfloat16)
            part = jnp.dot(probs, vx_ref[h, window, :], preferred_element_type=jnp.float32)
            acc = part if acc is None else acc + part
        att_ref[here, :] = acc.astype(jnp.bfloat16)
        return carry

    lax.fori_loop(0, rows // WINDOW, step, 0)
    for k, out in enumerate((t0_ref, t1_ref, t2_ref, t3_ref)):
        cols = pl.ds(pl.multiple_of(at_ref[NY + k] * span, span), span)
        out[...] = jnp.dot(
            att_ref[...], w_ref[:, cols], preferred_element_type=jnp.float32
        ).astype(jnp.bfloat16)


def vmem_specs(count):
    return [pl.BlockSpec(memory_space=pltpu.VMEM)] * count


def smem_specs(count):
    return [pl.BlockSpec(memory_space=pltpu.SMEM)] * count


def attention(order, sink, queries, keys_t, vals_t, labels, low, high, w_out):
    rows, cols = queries.shape
    span = w_out.shape[1] // (NY * NC)
    block = jax.ShapeDtypeStruct((rows, span), jnp.bfloat16)
    reach = rows + 2 * WINDOW
    heads = cols // HEAD_DIM
    return pl.pallas_call(
        attention_kernel,
        out_shape=[jax.ShapeDtypeStruct((rows, cols), jnp.bfloat16)] + [block] * NY,
        in_specs=smem_specs(2) + vmem_specs(7),
        out_specs=vmem_specs(1 + NY),
        scratch_shapes=[
            pltpu.VMEM((heads, cols, reach), jnp.bfloat16),
            pltpu.VMEM((heads, reach, cols), jnp.bfloat16),
            pltpu.VMEM((8, reach), jnp.float32),
            pltpu.VMEM((rows, WINDOW), jnp.float32),
        ],
        compiler_params=pltpu.CompilerParams(vmem_limit_bytes=20 * MB),
        cost_estimate=pl.CostEstimate(flops=4 * 10**9, bytes_accessed=4 * MB, transcendentals=0),
        name="attention",
    )(order, sink, queries, keys_t, vals_t, labels, low, high, w_out)


def pair_kernel(at_ref, left_ref, w_ref, g0, g1, g2, g3, s0, s1, s2, s3):
    span = g0.shape[1]
    for k, (got, out) in enumerate(((g0, s0), (g1, s1), (g2, s2), (g3, s3))):
        cols = pl.ds(pl.multiple_of(at_ref[k] * span, span), span)
        out[...] = (
            jnp.dot(left_ref[...], w_ref[:, cols], preferred_element_type=jnp.float32)
            + got[...].astype(jnp.float32)
        ).astype(jnp.bfloat16)


def pair_sums(order, left, w_out, got):
    return pl.pallas_call(
        pair_kernel,
        out_shape=[jax.ShapeDtypeStruct(got[0].shape, jnp.bfloat16)] * NY,
        in_specs=smem_specs(1) + vmem_specs(2 + NY),
        out_specs=vmem_specs(NY),
        compiler_params=pltpu.CompilerParams(vmem_limit_bytes=16 * MB),
        cost_estimate=pl.CostEstimate(flops=10**9, bytes_accessed=4 * MB, transcendentals=0),
        name="pair_sums",
    )(order, left, w_out, *got)


def to_owners(pairs):
    return [lax.ppermute(pairs[k], "tp", tp_shift(k, 0)) for k in range(1, NY)]


def per_device(
    queries,
    key_rows,
    values,
    sink_logits,
    doc_ids,
    residual,
    w_out,
    norm_gain,
    w_value_up,
    w_gate_up,
    conv_taps,
    w_down_t,
):
    rows_here = queries.shape[0]
    model_width = residual.shape[1]
    span = model_width // (NY * NC)
    ff = w_value_up.shape[1]
    sp, tp = lax.axis_index("sp"), lax.axis_index("tp")
    z, x, y, core = sp // NX, sp % NX, tp // NC, tp % NC
    toward = 1 - 2 * core
    order = jnp.stack(
        [((y + k) % NY) * NC + who for who in (core, 1 - core) for k in range(NY)]
    )
    count = lax.axis_size("sp")
    forward = [(i, i + 1) for i in range(count - 1)]
    backward = [(target, source) for source, target in forward]

    keys_t, vals_t = key_rows.T, values.T
    labels = (doc_ids + 1).astype(jnp.float32)[None, :]
    packed = jnp.concatenate([keys_t, vals_t, labels.astype(jnp.bfloat16)], axis=0)
    low = lax.ppermute(packed[:, -WINDOW:], "sp", forward)
    high = lax.ppermute(packed[:, :WINDOW], "sp", backward)

    tail = ff - ff % 128
    cut = 384
    share_a = jnp.concatenate([w_value_up, w_gate_up[:, tail:], w_gate_up[:, :cut]], axis=1)
    share_b = jnp.concatenate([w_gate_up[:, cut:tail], w_down_t], axis=1)
    rows_w, width_a = share_a.shape
    width_b = share_b.shape[1]
    other_a, other_b = swap(share_a), swap(share_b)

    def both(mine, other):
        out = jnp.zeros((NC,) + mine.shape, mine.dtype)
        return put(put(out, mine, core), other, 1 - core)

    both_a, both_b = both(share_a, other_a), both(share_b, other_b)
    near_a = send_apart(both_a, 0, 1)
    far_a = send_apart(share_a, 0, 2)
    step_b = send_apart(both_b, 1, 0)

    attended, *theirs = attention(
        order, sink_logits, queries, keys_t, vals_t, labels, low, high, w_out
    )
    got = [swap(block) for block in theirs]

    near_a2, far_a2 = swap(near_a), swap(far_a)
    block_a = jnp.zeros((NC, NX, rows_w, width_a), share_a.dtype)
    block_a = put(block_a, both_a[:, None], 0, x)
    block_a = put(block_a, near_a[:, None], 0, (x - toward) % NX)
    block_a = put(block_a, near_a2[:, None], 0, (x + toward) % NX)
    block_a = put(block_a, far_a, core, (x + 2) % NX)
    block_a = put(block_a, far_a2, 1 - core, (x + 2) % NX)
    block_a = block_a.reshape(NC, NX * rows_w, width_a)

    full_a = jnp.zeros((NZ, NX * rows_w, width_a), share_a.dtype)
    full_a = put(full_a, pick(block_a, core), z)
    whole_b = jnp.zeros((NC, NZ, rows_w, width_b), share_b.dtype)
    whole_b = put(whole_b, both_b[:, None], 0, z)

    def keep_a(full, step, k):
        full = put(full, pick(step, core), (z - toward * k) % NZ)
        return put(full, swap(pick(step, 1 - core)), (z + toward * k) % NZ)

    def keep_b(whole, step, k):
        whole = put(whole, step[:, None], 0, (z - toward * k) % NZ)
        return put(whole, swap(step)[:, None], 0, (z + toward * k) % NZ)

    step_a = send_apart(block_a, 1, 0)
    step_b2 = send_apart(step_b, 1, 0)
    whole_b = keep_b(whole_b, step_b, 1)

    pairs = pair_sums(order, attended, w_out, got)
    sent = to_owners(pairs)

    step_b3 = send_apart(after(step_b2, pairs[1]), 1, 0)
    whole_b = keep_b(whole_b, step_b2, 2)
    step_a2 = send_apart(after(step_a, pairs[1]), 1, 0)
    full_a = keep_a(full_a, step_a, 1)
    step_b4 = send_apart(pick(step_b3, core), 1, 0)
    whole_b = keep_b(whole_b, step_b3, 3)
    whole_b = put(whole_b, step_b4, core, (z + NZ // 2) % NZ)
    whole_b = put(whole_b, swap(step_b4), 1 - core, (z + NZ // 2) % NZ)
    near_b = send_apart(whole_b, 0, 1)
    far_b = send_apart(pick(whole_b, core), 0, 2)

    own_res = lax.dynamic_slice_in_dim(residual, tp * span, span, 1)
    total = own_res.astype(jnp.float32)
    summed = pairs[0].astype(jnp.float32)
    for block in sent:
        summed = summed + block.astype(jnp.float32)
    mixed_own = (total + summed).astype(jnp.bfloat16)

    parts = [mixed_own] + to_owners([mixed_own] * NY)
    others = [swap(part) for part in parts]

    step_a3 = send_apart(after(step_a2, mixed_own), 1, 0)
    full_a = keep_a(full_a, step_a2, 2)
    step_a4 = send_apart(pick(step_a3, core), 1, 0)
    full_a = keep_a(full_a, step_a3, 3)
    full_a = put(full_a, step_a4, (z + NZ // 2) % NZ).reshape(model_width, width_a)

    full_b = jnp.zeros((NZ, NX, rows_w, width_b), share_b.dtype)
    full_b = put(full_b, pick(whole_b, core)[:, None], 0, x)
    full_b = put(full_b, pick(near_b, core)[:, None], 0, (x - toward) % NX)
    full_b = put(full_b, swap(pick(near_b, 1 - core))[:, None], 0, (x + toward) % NX)
    full_b = put(full_b, far_b[:, None], 0, (x + 2) % NX).reshape(model_width, width_b)

    mixed = jnp.zeros((rows_here, model_width), jnp.bfloat16)
    for k in range(NY):
        at = ((y - k) % NY) * NC
        mixed = lax.dynamic_update_slice(mixed, parts[k], (0, (at + core) * span))
        mixed = lax.dynamic_update_slice(mixed, others[k], (0, (at + 1 - core) * span))
    mixed_f = mixed.astype(jnp.float32)
    mean_sq = jnp.mean(mixed_f * mixed_f, axis=1, keepdims=True)
    normed = (mixed_f * lax.rsqrt(mean_sq + EPS) * norm_gain).astype(jnp.bfloat16)

    up_a = jnp.dot(normed, full_a, preferred_element_type=jnp.float32).astype(jnp.bfloat16)
    up_b = jnp.dot(normed, full_b[:, : tail - cut], preferred_element_type=jnp.float32).astype(
        jnp.bfloat16
    )
    full_down = full_b[:, tail - cut :]
    up_value = up_a[:, :ff]
    up_gate = jnp.concatenate([up_a[:, ff + ff - tail :], up_b, up_a[:, ff : ff + ff - tail]], axis=1)
    before = lax.ppermute(up_value[-1:], "sp", forward)
    behind = lax.ppermute(up_value[:1], "sp", backward)
    rim_value = jnp.concatenate([before, up_value, behind], axis=0).astype(jnp.float32)
    edge = jnp.concatenate([low[-1:, -1:], packed[-1:], high[-1:, :1]], axis=1)[0]
    prev_same = (edge[:-2] == edge[1:-1])[:, None]
    next_same = (edge[2:] == edge[1:-1])[:, None]
    tap_f = conv_taps.astype(jnp.float32)
    conv = (
        tap_f[0] * jnp.where(prev_same, rim_value[:-2], 0.0)
        + tap_f[1] * up_value.astype(jnp.float32)
        + tap_f[2] * jnp.where(next_same, rim_value[2:], 0.0)
    )
    hidden = (jax.nn.silu(conv) * up_gate.astype(jnp.float32)).astype(jnp.bfloat16)

    def down(who):
        weights = jnp.concatenate(
            [
                lax.dynamic_slice_in_dim(full_down, (((y + k) % NY) * NC + who) * span, span, 0)
                for k in range(NY)
            ],
            axis=0,
        )
        out = lax.dot_general(
            hidden, weights, (((1,), (1,)), ((), ())), preferred_element_type=jnp.float32
        )
        return [out[:, k * span : (k + 1) * span] for k in range(NY)]

    got = [swap(block.astype(jnp.bfloat16)) for block in down(1 - core)]
    pairs = [
        (mine + theirs.astype(jnp.float32)).astype(jnp.bfloat16)
        for mine, theirs in zip(down(core), got)
    ]
    ffn_cols = pairs[0].astype(jnp.float32)
    for block in to_owners(pairs):
        ffn_cols = ffn_cols + block.astype(jnp.float32)
    return (mixed_own.astype(jnp.float32) + ffn_cols).astype(jnp.bfloat16)


def solution(mesh):
    placed = (
        P("sp", "tp"),
        P("sp", "tp"),
        P("sp", "tp"),
        P("tp"),
        P("sp"),
        P("sp", None),
        P("tp", None),
        P(),
        P("sp", "tp"),
        P("sp", "tp"),
        P(None, "tp"),
        P("sp", "tp"),
    )
    return jax.shard_map(
        per_device, mesh=mesh, in_specs=placed, out_specs=P("sp", "tp"), check_vma=False
    )
```

```python
import jax
import jax.numpy as jnp
from jax import lax
from jax.experimental import pallas as pl
from jax.experimental.pallas import tpu as pltpu
from jax.sharding import Mesh
from jax.sharding import PartitionSpec as P

HEAD_DIM = 64
WINDOW = 128
EPS = 1e-06
NEG = -1e30

NZ, NX, NY, NC = 8, 4, 4, 2
AXES = ("z", "x", "y", "core")
MB = 1 << 20


def shift_x(k):
    return [(x, (x + k) % NX) for x in range(NX)]


def swap(block):
    return lax.ppermute(block, "core", [(0, 1), (1, 0)])


def after(value, *others):
    return lax.optimization_barrier((value,) + others)[0]


def put(block, piece, *at):
    piece = piece.reshape((1,) * (block.ndim - piece.ndim) + piece.shape)
    start = list(at) + [0] * (block.ndim - len(at))
    return lax.dynamic_update_slice(block, piece, start)


def attention_kernel(
    at_ref, sink_ref, q_ref, kt_ref, vt_ref, lab_ref, low_ref, high_ref, w_ref,
    att_ref, theirs_ref, kx_ref, vx_ref, row_ref, col_ref,
):
    rows = q_ref.shape[0]
    heads = q_ref.shape[1] // HEAD_DIM
    span = theirs_ref.shape[2]
    kx_ref[...] = jnp.zeros_like(kx_ref)
    vx_ref[...] = jnp.zeros_like(vx_ref)
    pieces = (
        (0, WINDOW, low_ref[:HEAD_DIM], low_ref[HEAD_DIM : 2 * HEAD_DIM]),
        (WINDOW, rows, kt_ref[...], vt_ref[...]),
        (WINDOW + rows, WINDOW, high_ref[:HEAD_DIM], high_ref[HEAD_DIM : 2 * HEAD_DIM]),
    )
    for start, width, keys, vals in pieces:
        vals_t = vals.astype(jnp.float32).T.astype(jnp.bfloat16)
        for h in range(heads):
            kx_ref[h, h * HEAD_DIM : (h + 1) * HEAD_DIM, start : start + width] = keys
            vx_ref[h, start : start + width, h * HEAD_DIM : (h + 1) * HEAD_DIM] = vals_t
    row_ref[:, :WINDOW] = jnp.broadcast_to(
        low_ref[2 * HEAD_DIM :].astype(jnp.float32), (8, WINDOW)
    )
    row_ref[:, WINDOW : WINDOW + rows] = jnp.broadcast_to(lab_ref[...], (8, rows))
    row_ref[:, WINDOW + rows :] = jnp.broadcast_to(
        high_ref[2 * HEAD_DIM :].astype(jnp.float32), (8, WINDOW)
    )
    for n in range(rows // WINDOW):
        part = row_ref[:, (n + 1) * WINDOW : (n + 2) * WINDOW]
        col_ref[n * WINDOW : (n + 1) * WINDOW, :] = jnp.broadcast_to(
            part[:1], (WINDOW, WINDOW)
        ).T

    def step(n, carry):
        base = pl.multiple_of(n * WINDOW, WINDOW)
        here = pl.ds(base, WINDOW)
        window = pl.ds(base, 3 * WINDOW)
        q = q_ref[here, :] * jnp.bfloat16(HEAD_DIM ** (-0.5))
        offsets = (
            lax.broadcasted_iota(jnp.int32, (WINDOW, 3 * WINDOW), 1)
            - WINDOW
            - lax.broadcasted_iota(jnp.int32, (WINDOW, 3 * WINDOW), 0)
        )
        mine = col_ref[here, :1]
        allowed = (jnp.abs(offsets) <= WINDOW) & (row_ref[:1, window] == mine)
        acc = None
        for h in range(heads):
            score = jnp.dot(q, kx_ref[h, :, window], preferred_element_type=jnp.float32)
            score = jnp.where(allowed, score, NEG)
            highest = jnp.maximum(jnp.max(score, axis=1, keepdims=True), sink_ref[h])
            raw = jnp.exp(score - highest)
            total = jnp.sum(raw, axis=1, keepdims=True) + jnp.exp(sink_ref[h] - highest)
            probs = (raw * (1.0 / total)).astype(jnp.bfloat16)
            part = jnp.dot(probs, vx_ref[h, window, :], preferred_element_type=jnp.float32)
            acc = part if acc is None else acc + part
        att_ref[here, :] = acc.astype(jnp.bfloat16)
        return carry

    lax.fori_loop(0, rows // WINDOW, step, 0)
    for k in range(NY):
        cols = pl.ds(pl.multiple_of(at_ref[NY + k] * span, span), span)
        theirs_ref[k] = jnp.dot(
            att_ref[...], w_ref[:, cols], preferred_element_type=jnp.float32
        ).astype(jnp.bfloat16)


def vmem_specs(count):
    return [pl.BlockSpec(memory_space=pltpu.VMEM)] * count


def smem_specs(count):
    return [pl.BlockSpec(memory_space=pltpu.SMEM)] * count


def attention(order, sink, queries, keys_t, vals_t, labels, low, high, w_out):
    rows, cols = queries.shape
    span = w_out.shape[1] // (NY * NC)
    reach = rows + 2 * WINDOW
    heads = cols // HEAD_DIM
    return pl.pallas_call(
        attention_kernel,
        out_shape=[
            jax.ShapeDtypeStruct((rows, cols), jnp.bfloat16),
            jax.ShapeDtypeStruct((NY, rows, span), jnp.bfloat16),
        ],
        in_specs=smem_specs(2) + vmem_specs(7),
        out_specs=vmem_specs(2),
        scratch_shapes=[
            pltpu.VMEM((heads, cols, reach), jnp.bfloat16),
            pltpu.VMEM((heads, reach, cols), jnp.bfloat16),
            pltpu.VMEM((8, reach), jnp.float32),
            pltpu.VMEM((rows, WINDOW), jnp.float32),
        ],
        compiler_params=pltpu.CompilerParams(vmem_limit_bytes=12 * MB),
        cost_estimate=pl.CostEstimate(flops=4 * 10**9, bytes_accessed=4 * MB, transcendentals=0),
        name="attention",
    )(order, sink, queries, keys_t, vals_t, labels, low, high, w_out)


def pair_kernel(at_ref, left_ref, w_ref, got_ref, s0, s1, s2, s3):
    span = s0.shape[1]
    for k, out in enumerate((s0, s1, s2, s3)):
        cols = pl.ds(pl.multiple_of(at_ref[k] * span, span), span)
        out[...] = (
            jnp.dot(left_ref[...], w_ref[:, cols], preferred_element_type=jnp.float32)
            + got_ref[k].astype(jnp.float32)
        ).astype(jnp.bfloat16)


def pair_sums(order, left, w_out, got):
    return pl.pallas_call(
        pair_kernel,
        out_shape=[jax.ShapeDtypeStruct(got.shape[1:], jnp.bfloat16)] * NY,
        in_specs=smem_specs(1) + vmem_specs(3),
        out_specs=vmem_specs(NY),
        compiler_params=pltpu.CompilerParams(vmem_limit_bytes=8 * MB),
        cost_estimate=pl.CostEstimate(flops=10**9, bytes_accessed=4 * MB, transcendentals=0),
        name="pair_sums",
    )(order, left, w_out, got)


def to_owners(pairs):
    return [lax.ppermute(pairs[k], "y", [(y, (y + k) % NY) for y in range(NY)]) for k in range(1, NY)]


def per_device(
    queries,
    key_rows,
    values,
    sink_logits,
    doc_ids,
    residual,
    w_out,
    norm_gain,
    w_value_up,
    w_gate_up,
    conv_taps,
    w_down_t,
):
    rows_here = queries.shape[0]
    model_width = residual.shape[1]
    span = model_width // (NY * NC)
    ff = w_value_up.shape[1]
    _, x, y, core = (lax.axis_index(axis) for axis in AXES)
    tp = y * NC + core
    order = jnp.stack(
        [((y + k) % NY) * NC + who for who in (core, 1 - core) for k in range(NY)]
    )
    count = NZ * NX
    forward = [(i, i + 1) for i in range(count - 1)]
    backward = [(target, source) for source, target in forward]

    keys_t, vals_t = key_rows.T, values.T
    labels = (doc_ids + 1).astype(jnp.float32)[None, :]
    packed = jnp.concatenate([keys_t, vals_t, labels.astype(jnp.bfloat16)], axis=0)
    low = lax.ppermute(packed[:, -WINDOW:], ("z", "x"), forward)
    high = lax.ppermute(packed[:, :WINDOW], ("z", "x"), backward)

    share = jnp.concatenate([after(w_value_up, packed), w_gate_up, w_down_t], axis=1)
    rows_w, width = share.shape
    gathered = []
    for k in range(1, NX):
        gathered.append(lax.ppermute(share, "x", shift_x(k)))

    attended, theirs = attention(
        order, sink_logits, queries, keys_t, vals_t, labels, low, high, w_out
    )
    got = swap(theirs)

    block = put(jnp.zeros((NX, rows_w, width), share.dtype), share, x)
    gathered = lax.optimization_barrier((*gathered, theirs))[:-1]
    for k, piece in enumerate(gathered):
        block = put(block, piece, (x - k - 1) % NX)
    full = lax.all_gather(block.reshape(NX * rows_w, width), "z", axis=0, tiled=True)

    pairs = pair_sums(order, attended, w_out, got)
    sent = to_owners(pairs)

    own_res = lax.dynamic_slice_in_dim(residual, tp * span, span, 1)
    total = own_res.astype(jnp.float32)
    summed = pairs[0].astype(jnp.float32)
    for block in sent:
        summed = summed + block.astype(jnp.float32)
    mixed_own = (total + summed).astype(jnp.bfloat16)

    parts = [mixed_own] + to_owners([mixed_own] * NY)
    others = [swap(mixed_own)]
    rest = swap(jnp.stack(parts[1:]))
    others += [rest[k] for k in range(NY - 1)]

    mixed = jnp.zeros((rows_here, model_width), jnp.bfloat16)
    for k in range(NY):
        at = ((y - k) % NY) * NC
        mixed = lax.dynamic_update_slice(mixed, parts[k], (0, (at + core) * span))
        mixed = lax.dynamic_update_slice(mixed, others[k], (0, (at + 1 - core) * span))
    mixed_f = mixed.astype(jnp.float32)
    mean_sq = jnp.mean(mixed_f * mixed_f, axis=1, keepdims=True)
    normed = (mixed_f * lax.rsqrt(mean_sq + EPS) * norm_gain).astype(jnp.bfloat16)

    up_value = jnp.dot(normed, full[:, :ff], preferred_element_type=jnp.float32).astype(
        jnp.bfloat16
    )
    before = lax.ppermute(up_value[-1:], ("z", "x"), forward)
    behind = lax.ppermute(up_value[:1], ("z", "x"), backward)
    up_gate = after(
        jnp.dot(normed, full[:, ff : 2 * ff], preferred_element_type=jnp.float32).astype(
            jnp.bfloat16
        ),
        up_value,
    )
    rim_value = jnp.concatenate([before, up_value, behind], axis=0).astype(jnp.float32)
    edge = jnp.concatenate([low[-1:, -1:], packed[-1:], high[-1:, :1]], axis=1)[0]
    prev_same = (edge[:-2] == edge[1:-1])[:, None]
    next_same = (edge[2:] == edge[1:-1])[:, None]
    tap_f = conv_taps.astype(jnp.float32)
    conv = (
        tap_f[0] * jnp.where(prev_same, rim_value[:-2], 0.0)
        + tap_f[1] * up_value.astype(jnp.float32)
        + tap_f[2] * jnp.where(next_same, rim_value[2:], 0.0)
    )
    hidden = (jax.nn.silu(conv) * up_gate.astype(jnp.float32)).astype(jnp.bfloat16)

    def down(who):
        weights = jnp.concatenate(
            [
                lax.dynamic_slice(
                    full, ((((y + k) % NY) * NC + who) * span, 2 * ff), (span, ff)
                )
                for k in range(NY)
            ],
            axis=0,
        )
        return lax.dot_general(
            hidden, weights, (((1,), (1,)), ((), ())), preferred_element_type=jnp.float32
        )

    got = swap(down(1 - core).astype(jnp.bfloat16))
    pair = (down(core) + got.astype(jnp.float32)).astype(jnp.bfloat16)
    pairs = [pair[:, k * span : (k + 1) * span] for k in range(NY)]
    ffn_cols = pairs[0].astype(jnp.float32)
    for block in to_owners(pairs):
        ffn_cols = ffn_cols + block.astype(jnp.float32)
    return (mixed_own.astype(jnp.float32) + ffn_cols).astype(jnp.bfloat16)


def solution(mesh):
    grid = Mesh(mesh.devices.reshape(NZ, NX, NY, NC), AXES)
    sp, tp = ("z", "x"), ("y", "core")
    placed = (
        P(sp, tp),
        P(sp, tp),
        P(sp, tp),
        P(tp),
        P(sp),
        P(sp, None),
        P(tp, None),
        P(),
        P(sp, tp),
        P(sp, tp),
        P(None, tp),
        P(sp, tp),
    )
    return jax.shard_map(
        per_device, mesh=grid, in_specs=placed, out_specs=P(sp, tp), check_vma=False
    )
```

```python
import functools

import jax
import jax.numpy as jnp
from jax import lax
from jax.experimental import pallas as pl
from jax.experimental.pallas import tpu as pltpu
from jax.sharding import Mesh
from jax.sharding import PartitionSpec as P

HEAD_DIM = 64
WINDOW = 128
EPS = 1e-06
NEG = -1e30

NZ, NX, NY, NC = 8, 4, 4, 2
AXES = ("z", "x", "y", "core")
MB = 1 << 20


def index_of(z, x, y, c):
    return (((z % NZ) * NX + x % NX) * NY + y % NY) * NC + c


def send_apart(block, dz, dx):
    pairs = [
        (index_of(z, x, y, c), index_of(z + s * dz, x + s * dx, y, c))
        for z in range(NZ)
        for x in range(NX)
        for y in range(NY)
        for c, s in ((0, 1), (1, -1))
    ]
    return lax.ppermute(block, AXES, pairs)


def send_z(block, k):
    return lax.ppermute(block, "z", [(z, (z + k) % NZ) for z in range(NZ)])


def send_x(block, k):
    return lax.ppermute(block, "x", [(x, (x + k) % NX) for x in range(NX)])


def swap(block):
    return lax.ppermute(block, "core", [(0, 1), (1, 0)])


def after(value, *others):
    return lax.optimization_barrier((value,) + others)[0]


def put(block, piece, *at):
    piece = piece.reshape((1,) * (block.ndim - piece.ndim) + piece.shape)
    start = list(at) + [0] * (block.ndim - len(at))
    return lax.dynamic_update_slice(block, piece, start)


def attention_kernel(
    at_ref, sink_ref, q_ref, kt_ref, vt_ref, lab_ref, low_ref, high_ref, w_ref,
    att_ref, theirs_ref, kx_ref, vx_ref, row_ref, col_ref,
):
    rows = q_ref.shape[0]
    heads = q_ref.shape[1] // HEAD_DIM
    span = theirs_ref.shape[2]
    kx_ref[...] = jnp.zeros_like(kx_ref)
    vx_ref[...] = jnp.zeros_like(vx_ref)
    pieces = (
        (0, WINDOW, low_ref[:HEAD_DIM], low_ref[HEAD_DIM : 2 * HEAD_DIM]),
        (WINDOW, rows, kt_ref[...], vt_ref[...]),
        (WINDOW + rows, WINDOW, high_ref[:HEAD_DIM], high_ref[HEAD_DIM : 2 * HEAD_DIM]),
    )
    for start, width, keys, vals in pieces:
        vals_t = vals.astype(jnp.float32).T.astype(jnp.bfloat16)
        for h in range(heads):
            kx_ref[h, h * HEAD_DIM : (h + 1) * HEAD_DIM, start : start + width] = keys
            vx_ref[h, start : start + width, h * HEAD_DIM : (h + 1) * HEAD_DIM] = vals_t
    row_ref[:, :WINDOW] = jnp.broadcast_to(
        low_ref[2 * HEAD_DIM :].astype(jnp.float32), (8, WINDOW)
    )
    row_ref[:, WINDOW : WINDOW + rows] = jnp.broadcast_to(lab_ref[...], (8, rows))
    row_ref[:, WINDOW + rows :] = jnp.broadcast_to(
        high_ref[2 * HEAD_DIM :].astype(jnp.float32), (8, WINDOW)
    )
    for n in range(rows // WINDOW):
        part = row_ref[:, (n + 1) * WINDOW : (n + 2) * WINDOW]
        col_ref[n * WINDOW : (n + 1) * WINDOW, :] = jnp.broadcast_to(
            part[:1], (WINDOW, WINDOW)
        ).T

    def step(n, carry):
        base = pl.multiple_of(n * WINDOW, WINDOW)
        here = pl.ds(base, WINDOW)
        window = pl.ds(base, 3 * WINDOW)
        q = q_ref[here, :] * jnp.bfloat16(HEAD_DIM ** (-0.5))
        offsets = (
            lax.broadcasted_iota(jnp.int32, (WINDOW, 3 * WINDOW), 1)
            - WINDOW
            - lax.broadcasted_iota(jnp.int32, (WINDOW, 3 * WINDOW), 0)
        )
        mine = col_ref[here, :1]
        allowed = (jnp.abs(offsets) <= WINDOW) & (row_ref[:1, window] == mine)
        acc = None
        for h in range(heads):
            score = jnp.dot(q, kx_ref[h, :, window], preferred_element_type=jnp.float32)
            score = jnp.where(allowed, score, NEG)
            highest = jnp.maximum(jnp.max(score, axis=1, keepdims=True), sink_ref[h])
            raw = jnp.exp(score - highest)
            total = jnp.sum(raw, axis=1, keepdims=True) + jnp.exp(sink_ref[h] - highest)
            probs = (raw * (1.0 / total)).astype(jnp.bfloat16)
            part = jnp.dot(probs, vx_ref[h, window, :], preferred_element_type=jnp.float32)
            acc = part if acc is None else acc + part
        att_ref[here, :] = acc.astype(jnp.bfloat16)
        return carry

    lax.fori_loop(0, rows // WINDOW, step, 0)
    for k in range(NY):
        cols = pl.ds(pl.multiple_of(at_ref[NY + k] * span, span), span)
        theirs_ref[k] = jnp.dot(
            att_ref[...], w_ref[:, cols], preferred_element_type=jnp.float32
        ).astype(jnp.bfloat16)


def vmem_specs(count):
    return [pl.BlockSpec(memory_space=pltpu.VMEM)] * count


def smem_specs(count):
    return [pl.BlockSpec(memory_space=pltpu.SMEM)] * count


def attention(order, sink, queries, keys_t, vals_t, labels, low, high, w_out):
    rows, cols = queries.shape
    span = w_out.shape[1] // (NY * NC)
    reach = rows + 2 * WINDOW
    heads = cols // HEAD_DIM
    return pl.pallas_call(
        attention_kernel,
        out_shape=[
            jax.ShapeDtypeStruct((rows, cols), jnp.bfloat16),
            jax.ShapeDtypeStruct((NY, rows, span), jnp.bfloat16),
        ],
        in_specs=smem_specs(2) + vmem_specs(7),
        out_specs=vmem_specs(2),
        scratch_shapes=[
            pltpu.VMEM((heads, cols, reach), jnp.bfloat16),
            pltpu.VMEM((heads, reach, cols), jnp.bfloat16),
            pltpu.VMEM((8, reach), jnp.float32),
            pltpu.VMEM((rows, WINDOW), jnp.float32),
        ],
        compiler_params=pltpu.CompilerParams(vmem_limit_bytes=12 * MB),
        cost_estimate=pl.CostEstimate(flops=4 * 10**9, bytes_accessed=4 * MB, transcendentals=0),
        name="attention",
    )(order, sink, queries, keys_t, vals_t, labels, low, high, w_out)


def pair_kernel(at_ref, left_ref, w_ref, got_ref, s0, s1, s2, s3):
    span = s0.shape[1]
    for k, out in enumerate((s0, s1, s2, s3)):
        cols = pl.ds(pl.multiple_of(at_ref[k] * span, span), span)
        out[...] = (
            jnp.dot(left_ref[...], w_ref[:, cols], preferred_element_type=jnp.float32)
            + got_ref[k].astype(jnp.float32)
        ).astype(jnp.bfloat16)


def pair_sums(order, left, w_out, got):
    return pl.pallas_call(
        pair_kernel,
        out_shape=[jax.ShapeDtypeStruct(got.shape[1:], jnp.bfloat16)] * NY,
        in_specs=smem_specs(1) + vmem_specs(3),
        out_specs=vmem_specs(NY),
        compiler_params=pltpu.CompilerParams(vmem_limit_bytes=8 * MB),
        cost_estimate=pl.CostEstimate(flops=10**9, bytes_accessed=4 * MB, transcendentals=0),
        name="pair_sums",
    )(order, left, w_out, got)


def norm_kernel(at_ref, p0, p1, p2, p3, rest_ref, gain_ref, out_ref):
    rows, span = p0.shape
    width = out_ref.shape[1]

    def step(n, carry):
        here = pl.ds(pl.multiple_of(n * 64, 64), 64)
        mine = [ref[here, :].astype(jnp.float32) for ref in (p0, p1, p2, p3)]
        theirs = [rest_ref[k, here, :].astype(jnp.float32) for k in range(NY)]
        square = sum(block * block for block in mine + theirs)
        mean_sq = jnp.sum(square, axis=1, keepdims=True) * (1.0 / width)
        scale = lax.rsqrt(mean_sq + EPS)
        for k, block in enumerate(mine + theirs):
            cols = pl.ds(pl.multiple_of(at_ref[2 * NY + k] * span, span), span)
            out_ref[here, cols] = (block * scale * gain_ref[:, cols]).astype(jnp.bfloat16)
        return carry

    lax.fori_loop(0, rows // 64, step, 0)


def normalised(order, parts, rest, gain):
    rows, _ = parts[0].shape
    return pl.pallas_call(
        norm_kernel,
        out_shape=jax.ShapeDtypeStruct((rows, gain.shape[1]), jnp.bfloat16),
        in_specs=smem_specs(1) + vmem_specs(NY + 2),
        out_specs=pl.BlockSpec(memory_space=pltpu.VMEM),
        compiler_params=pltpu.CompilerParams(vmem_limit_bytes=10 * MB),
        cost_estimate=pl.CostEstimate(flops=2 * 10**9, bytes_accessed=6 * MB, transcendentals=0),
        name="normalise",
    )(order, *parts, rest, gain)


def up_kernel(start, left_ref, w_ref, out_ref):
    width = out_ref.shape[1]

    def step(n, carry):
        here = pl.ds(pl.multiple_of(n * 256, 256), 256)
        out_ref[here, :] = jnp.dot(
            left_ref[here, :], w_ref[:, start : start + width], preferred_element_type=jnp.float32
        ).astype(jnp.bfloat16)
        return carry

    lax.fori_loop(0, left_ref.shape[0] // 256, step, 0)


def up(left, weights, start, width):
    return pl.pallas_call(
        functools.partial(up_kernel, start),
        out_shape=jax.ShapeDtypeStruct((left.shape[0], width), jnp.bfloat16),
        in_specs=vmem_specs(2),
        out_specs=pl.BlockSpec(memory_space=pltpu.VMEM),
        compiler_params=pltpu.CompilerParams(vmem_limit_bytes=14 * MB),
        cost_estimate=pl.CostEstimate(flops=3 * 10**9, bytes_accessed=8 * MB, transcendentals=0),
    )(left, weights)


def hidden_kernel(value_ref, gate_ref, same_ref, before_ref, behind_ref, taps_ref, out_ref):
    rows, ff = out_ref.shape
    tail = gate_ref.shape[1]
    width = value_ref.shape[1]
    chunk = 64
    count = rows // chunk
    row = lax.broadcasted_iota(jnp.int32, (chunk, 128), 0)

    for at in range(0, width, 128):
        cols = slice(at, at + 128)
        if at < tail:
            low, high = before_ref[:, cols], behind_ref[:, cols]
            taps = taps_ref[:, cols].astype(jnp.float32)
        else:
            pad = ((0, 0), (0, at + 128 - ff))
            low, high = jnp.pad(before_ref[:, at:ff], pad), jnp.pad(behind_ref[:, at:ff], pad)
            taps = jnp.pad(taps_ref[:, at:ff].astype(jnp.float32), pad)
        low, high = low.astype(jnp.float32), high.astype(jnp.float32)

        def step(n, above):
            base = pl.multiple_of(n * chunk, chunk)
            here = pl.ds(base, chunk)
            value = value_ref[here, cols].astype(jnp.float32)
            following = pl.ds(pl.multiple_of(jnp.minimum(base + chunk, rows - 16), 16), 16)
            below = value_ref[following, cols].astype(jnp.float32)[:1]
            below = jnp.where(n == count - 1, high, below)
            prior = jnp.where(row == 0, above, pltpu.roll(value, 1, 0))
            after_ = jnp.where(row == chunk - 1, below, pltpu.roll(value, chunk - 1, 0))
            prev_same, next_same = same_ref[here, :1] > 0.5, same_ref[here, 1:2] > 0.5
            conv = (
                taps[0:1] * jnp.where(prev_same, prior, 0.0)
                + taps[1:2] * value
                + taps[2:3] * jnp.where(next_same, after_, 0.0)
            )
            act = conv * lax.logistic(conv)
            if at < tail:
                out_ref[here, cols] = (act * gate_ref[here, cols].astype(jnp.float32)).astype(
                    jnp.bfloat16
                )
            else:
                gate = pltpu.roll(value, 64, 1)
                out_ref[here, at:ff] = (act * gate).astype(jnp.bfloat16)[:, : ff - at]
            return value[chunk - 1 :]

        lax.fori_loop(0, count, step, low)


def hidden_units(value, gate, same, before, behind, taps):
    rows, ff = value.shape[0], taps.shape[1]
    return pl.pallas_call(
        hidden_kernel,
        out_shape=jax.ShapeDtypeStruct((rows, ff), jnp.bfloat16),
        in_specs=vmem_specs(6),
        out_specs=pl.BlockSpec(memory_space=pltpu.VMEM),
        compiler_params=pltpu.CompilerParams(vmem_limit_bytes=8 * MB),
        cost_estimate=pl.CostEstimate(flops=2 * 10**9, bytes_accessed=4 * MB, transcendentals=0),
        name="hidden_units",
    )(value, gate, same, before, behind, taps)


def to_owners(pairs):
    got = []
    for k in range(1, NY):
        got.append(lax.ppermute(pairs[k], "y", [(y, (y + k) % NY) for y in range(NY)]))
    return got


def per_device(
    queries,
    key_rows,
    values,
    sink_logits,
    doc_ids,
    residual,
    w_out,
    norm_gain,
    w_value_up,
    w_gate_up,
    conv_taps,
    w_down_t,
):
    model_width = residual.shape[1]
    span = model_width // (NY * NC)
    ff = w_value_up.shape[1]
    z, x, y, core = (lax.axis_index(axis) for axis in AXES)
    tp = y * NC + core
    order = jnp.stack(
        [((y + k) % NY) * NC + who for who in (core, 1 - core) for k in range(NY)]
        + [((y - k) % NY) * NC + who for who in (core, 1 - core) for k in range(NY)]
    )
    count = NZ * NX
    forward = [(i, i + 1) for i in range(count - 1)]
    backward = [(target, source) for source, target in forward]

    keys_t, vals_t = key_rows.T, values.T
    labels = (doc_ids + 1).astype(jnp.float32)[None, :]
    packed = jnp.concatenate([keys_t, vals_t, labels.astype(jnp.bfloat16)], axis=0)
    low = lax.ppermute(packed[:, -WINDOW:], ("z", "x"), forward)
    high = lax.ppermute(packed[:, :WINDOW], ("z", "x"), backward)

    tail = ff - ff % 128
    first = after(w_value_up, packed)
    share = jnp.concatenate(
        [w_gate_up[:, :tail], first, w_gate_up[:, tail:]], axis=1
    )
    rows_w, width = share.shape
    gathered = []
    for k in range(1, NX):
        gathered.append(send_x(share, k))

    attended, theirs = attention(
        order, sink_logits, queries, keys_t, vals_t, labels, low, high, w_out
    )
    got = swap(theirs)

    gathered = lax.optimization_barrier((*gathered, theirs))[:-1]
    block = put(jnp.zeros((NX, rows_w, width), share.dtype), share, x)
    for k, piece in enumerate(gathered):
        block = put(block, piece, (x - k - 1) % NX)
    block = block.reshape(NX * rows_w, width)
    full = put(jnp.zeros((NZ, NX * rows_w, width), share.dtype), block, z)

    def ring_step(plus, minus):
        plus = send_z(plus, 1)
        minus = send_z(minus, -1)
        return plus, minus

    def keep(full, plus, minus, k):
        return put(put(full, plus, (z - k) % NZ), minus, (z + k) % NZ)

    plus1, minus1 = ring_step(block, block)

    pairs = pair_sums(order, attended, w_out, got)
    sent = to_owners(pairs)

    down1 = after(w_down_t, pairs[0])
    near = ring_step(down1, down1)
    far_plus = send_z(down1, 2)
    far_minus = send_z(down1, -2)

    plus2, minus2 = ring_step(plus1, minus1)
    third = ring_step(far_plus, far_minus)
    last = send_apart(jnp.where(core == 0, far_plus, far_minus), 2, 0)
    whole = put(jnp.zeros((NZ,) + w_down_t.shape, w_down_t.dtype), w_down_t, z)
    whole = keep(whole, *near, 1)
    whole = keep(whole, far_plus, far_minus, 2)
    whole = keep(whole, *third, 3)
    whole = put(whole, last, (z + NZ // 2) % NZ)

    own_res = lax.dynamic_slice_in_dim(residual, tp * span, span, 1)
    total = own_res.astype(jnp.float32)
    summed = pairs[0].astype(jnp.float32)
    for block in sent:
        summed = summed + block.astype(jnp.float32)
    mixed_own = (total + summed).astype(jnp.bfloat16)

    parts = [mixed_own] + to_owners([mixed_own] * NY)
    plus3, minus3 = ring_step(plus2, minus2)
    full = keep(after(full, mixed_own), plus1, minus1, 1)
    whole_plus = send_x(whole, 1)
    whole_minus = send_x(whole, -1)

    rest = swap(jnp.stack(parts))
    last = send_apart(jnp.where(core == 0, plus3, minus3), 1, 0)
    full = keep(after(full, rest), plus2, minus2, 2)
    full = keep(full, plus3, minus3, 3)
    full = put(full, last, (z + NZ // 2) % NZ).reshape(model_width, width)

    whole_far = send_apart(jnp.where(core == 0, whole_plus, whole_minus), 0, 1)
    full_down = jnp.zeros((NZ, NX, rows_w, ff), w_down_t.dtype)
    full_down = put(full_down, whole[:, None], 0, x)
    full_down = put(full_down, whole_plus[:, None], 0, (x - 1) % NX)
    full_down = put(full_down, whole_minus[:, None], 0, (x + 1) % NX)
    full_down = put(full_down, whole_far[:, None], 0, (x + 2) % NX).reshape(model_width, ff)

    normed = normalised(order, parts, rest, norm_gain[None])
    up_value = up(normed, full, tail, width - tail)
    before = lax.ppermute(up_value[-1:, :ff], ("z", "x"), forward)
    behind = lax.ppermute(up_value[:1, :ff], ("z", "x"), backward)
    up_gate = up(normed, full, 0, tail)
    edge = jnp.concatenate([low[-1:, -1:], packed[-1:], high[-1:, :1]], axis=1)[0]
    same = jnp.stack([edge[:-2] == edge[1:-1], edge[2:] == edge[1:-1]], axis=1)
    same = same.astype(jnp.float32)
    hidden = hidden_units(up_value, up_gate, same, before, behind, conv_taps)

    def down(who):
        weights = jnp.concatenate(
            [
                lax.dynamic_slice(
                    full_down, ((((y + k) % NY) * NC + who) * span, 0), (span, ff)
                )
                for k in range(NY)
            ],
            axis=0,
        )
        return lax.dot_general(
            hidden, weights, (((1,), (1,)), ((), ())), preferred_element_type=jnp.float32
        )

    got = swap(down(1 - core).astype(jnp.bfloat16))
    pair = (down(core) + got.astype(jnp.float32)).astype(jnp.bfloat16)
    pairs = [pair[:, k * span : (k + 1) * span] for k in range(NY)]
    ffn_cols = pairs[0].astype(jnp.float32)
    for block in to_owners(pairs):
        ffn_cols = ffn_cols + block.astype(jnp.float32)
    return (mixed_own.astype(jnp.float32) + ffn_cols).astype(jnp.bfloat16)


def solution(mesh):
    grid = Mesh(mesh.devices.reshape(NZ, NX, NY, NC), AXES)
    sp, tp = ("z", "x"), ("y", "core")
    placed = (
        P(sp, tp),
        P(sp, tp),
        P(sp, tp),
        P(tp),
        P(sp),
        P(sp, None),
        P(tp, None),
        P(),
        P(sp, tp),
        P(sp, tp),
        P(None, tp),
        P(sp, tp),
    )
    return jax.shard_map(
        per_device, mesh=grid, in_specs=placed, out_specs=P(sp, tp), check_vma=False
    )
```

```python
import functools

import jax
import jax.numpy as jnp
from jax import lax
from jax.experimental import pallas as pl
from jax.experimental.pallas import tpu as pltpu
from jax.sharding import Mesh
from jax.sharding import PartitionSpec as P

HEAD_DIM = 64
WINDOW = 128
EPS = 1e-06
NEG = -1e30

NZ, NX, NY, NC = 8, 4, 4, 2
AXES = ("z", "x", "y", "core")
MB = 1 << 20


def index_of(z, x, y, c):
    return (((z % NZ) * NX + x % NX) * NY + y % NY) * NC + c


def send_apart(block, dz, dx):
    pairs = [
        (index_of(z, x, y, c), index_of(z + s * dz, x + s * dx, y, c))
        for z in range(NZ)
        for x in range(NX)
        for y in range(NY)
        for c, s in ((0, 1), (1, -1))
    ]
    return lax.ppermute(block, AXES, pairs)


def send_z(block, k):
    return lax.ppermute(block, "z", [(z, (z + k) % NZ) for z in range(NZ)])


def send_x(block, k):
    return lax.ppermute(block, "x", [(x, (x + k) % NX) for x in range(NX)])


def swap(block):
    return lax.ppermute(block, "core", [(0, 1), (1, 0)])


def after(value, *others):
    return lax.optimization_barrier((value,) + others)[0]


def put(block, piece, *at):
    piece = piece.reshape((1,) * (block.ndim - piece.ndim) + piece.shape)
    start = list(at) + [0] * (block.ndim - len(at))
    return lax.dynamic_update_slice(block, piece, start)


def attention_kernel(
    at_ref, sink_ref, q_hbm, w_hbm, packed_ref, low_ref, high_ref,
    theirs_ref, mine_ref,
    q_ref, w_ref, att_ref, kx_ref, vx_ref, row_ref, col_ref, sems,
):
    copies = [
        pltpu.make_async_copy(source, target, sems.at[i])
        for i, (source, target) in enumerate(
            ((q_hbm, q_ref), (w_hbm, w_ref))
        )
    ]
    for copy in copies:
        copy.start()
    rows = q_ref.shape[0]
    heads = q_ref.shape[1] // HEAD_DIM
    span = theirs_ref.shape[2]
    kx_ref[...] = jnp.zeros_like(kx_ref)
    vx_ref[...] = jnp.zeros_like(vx_ref)
    copies[0].wait()
    pieces = (
        (0, WINDOW, low_ref[:HEAD_DIM], low_ref[HEAD_DIM : 2 * HEAD_DIM]),
        (WINDOW, rows, packed_ref[:HEAD_DIM], packed_ref[HEAD_DIM : 2 * HEAD_DIM]),
        (WINDOW + rows, WINDOW, high_ref[:HEAD_DIM], high_ref[HEAD_DIM : 2 * HEAD_DIM]),
    )
    for start, width, keys, vals in pieces:
        vals_t = vals.astype(jnp.float32).T.astype(jnp.bfloat16)
        for h in range(heads):
            kx_ref[h, h * HEAD_DIM : (h + 1) * HEAD_DIM, start : start + width] = keys
            vx_ref[h, start : start + width, h * HEAD_DIM : (h + 1) * HEAD_DIM] = vals_t
    row_ref[:, :WINDOW] = jnp.broadcast_to(
        low_ref[2 * HEAD_DIM :].astype(jnp.float32), (8, WINDOW)
    )
    row_ref[:, WINDOW : WINDOW + rows] = jnp.broadcast_to(
        packed_ref[2 * HEAD_DIM :].astype(jnp.float32), (8, rows)
    )
    row_ref[:, WINDOW + rows :] = jnp.broadcast_to(
        high_ref[2 * HEAD_DIM :].astype(jnp.float32), (8, WINDOW)
    )
    for n in range(rows // WINDOW):
        part = row_ref[:, (n + 1) * WINDOW : (n + 2) * WINDOW]
        col_ref[n * WINDOW : (n + 1) * WINDOW, :] = jnp.broadcast_to(
            part[:1], (WINDOW, WINDOW)
        ).T

    def step(n, carry):
        base = pl.multiple_of(n * WINDOW, WINDOW)
        here = pl.ds(base, WINDOW)
        window = pl.ds(base, 3 * WINDOW)
        q = q_ref[here, :] * jnp.bfloat16(HEAD_DIM ** (-0.5))
        offsets = (
            lax.broadcasted_iota(jnp.int32, (WINDOW, 3 * WINDOW), 1)
            - WINDOW
            - lax.broadcasted_iota(jnp.int32, (WINDOW, 3 * WINDOW), 0)
        )
        mine = col_ref[here, :1]
        allowed = (jnp.abs(offsets) <= WINDOW) & (row_ref[:1, window] == mine)
        acc = None
        for h in range(heads):
            score = jnp.dot(q, kx_ref[h, :, window], preferred_element_type=jnp.float32)
            score = jnp.where(allowed, score, NEG)
            highest = jnp.maximum(jnp.max(score, axis=1, keepdims=True), sink_ref[h])
            raw = jnp.exp(score - highest)
            total = jnp.sum(raw, axis=1, keepdims=True) + jnp.exp(sink_ref[h] - highest)
            probs = (raw * (1.0 / total)).astype(jnp.bfloat16)
            part = jnp.dot(probs, vx_ref[h, window, :], preferred_element_type=jnp.float32)
            acc = part if acc is None else acc + part
        att_ref[here, :] = acc.astype(jnp.bfloat16)
        return carry

    lax.fori_loop(0, rows // WINDOW, step, 0)
    copies[1].wait()
    for k in range(NY):
        cols = pl.ds(pl.multiple_of(at_ref[NY + k] * span, span), span)
        theirs_ref[k] = jnp.dot(
            att_ref[...], w_ref[:, cols], preferred_element_type=jnp.float32
        ).astype(jnp.bfloat16)
        cols = pl.ds(pl.multiple_of(at_ref[k] * span, span), span)
        mine_ref[k] = jnp.dot(att_ref[...], w_ref[:, cols], preferred_element_type=jnp.float32)


def vmem_specs(count):
    return [pl.BlockSpec(memory_space=pltpu.VMEM)] * count


def smem_specs(count):
    return [pl.BlockSpec(memory_space=pltpu.SMEM)] * count


def attention(order, sink, queries, packed, low, high, w_out):
    rows, cols = queries.shape
    span = w_out.shape[1] // (NY * NC)
    reach = rows + 2 * WINDOW
    heads = cols // HEAD_DIM
    return pl.pallas_call(
        attention_kernel,
        out_shape=[
            jax.ShapeDtypeStruct((NY, rows, span), jnp.bfloat16),
            jax.ShapeDtypeStruct((NY, rows, span), jnp.float32),
        ],
        in_specs=smem_specs(2) + [pl.BlockSpec(memory_space=pltpu.HBM)] * 2 + vmem_specs(3),
        out_specs=vmem_specs(2),
        scratch_shapes=[
            pltpu.VMEM((rows, cols), jnp.bfloat16),
            pltpu.VMEM(w_out.shape, jnp.bfloat16),
            pltpu.VMEM((rows, cols), jnp.bfloat16),
            pltpu.VMEM((heads, cols, reach), jnp.bfloat16),
            pltpu.VMEM((heads, reach, cols), jnp.bfloat16),
            pltpu.VMEM((8, reach), jnp.float32),
            pltpu.VMEM((rows, WINDOW), jnp.float32),
            pltpu.SemaphoreType.DMA((2,)),
        ],
        compiler_params=pltpu.CompilerParams(vmem_limit_bytes=12 * MB),
        cost_estimate=pl.CostEstimate(flops=4 * 10**9, bytes_accessed=4 * MB, transcendentals=0),
        name="attention",
    )(order, sink, queries, w_out, packed, low, high)


def pair_kernel(mine_ref, got_ref, s0, s1, s2, s3):
    for k, out in enumerate((s0, s1, s2, s3)):
        out[...] = (mine_ref[k] + got_ref[k].astype(jnp.float32)).astype(jnp.bfloat16)


def pair_sums(mine, got):
    return pl.pallas_call(
        pair_kernel,
        out_shape=[jax.ShapeDtypeStruct(got.shape[1:], jnp.bfloat16)] * NY,
        in_specs=vmem_specs(2),
        out_specs=vmem_specs(NY),
        compiler_params=pltpu.CompilerParams(vmem_limit_bytes=8 * MB),
        cost_estimate=pl.CostEstimate(flops=10**9, bytes_accessed=4 * MB, transcendentals=0),
        name="pair_sums",
    )(mine, got)


def norm_kernel(at_ref, p0, p1, p2, p3, rest_ref, gain_ref, out_ref):
    rows, span = p0.shape
    width = out_ref.shape[1]

    def step(n, carry):
        here = pl.ds(pl.multiple_of(n * 64, 64), 64)
        mine = [ref[here, :].astype(jnp.float32) for ref in (p0, p1, p2, p3)]
        theirs = [rest_ref[k, here, :].astype(jnp.float32) for k in range(NY)]
        square = sum(block * block for block in mine + theirs)
        mean_sq = jnp.sum(square, axis=1, keepdims=True) * (1.0 / width)
        scale = lax.rsqrt(mean_sq + EPS)
        for k, block in enumerate(mine + theirs):
            cols = pl.ds(pl.multiple_of(at_ref[2 * NY + k] * span, span), span)
            out_ref[here, cols] = (block * scale * gain_ref[:, cols]).astype(jnp.bfloat16)
        return carry

    lax.fori_loop(0, rows // 64, step, 0)


def normalised(order, parts, rest, gain):
    rows, _ = parts[0].shape
    return pl.pallas_call(
        norm_kernel,
        out_shape=jax.ShapeDtypeStruct((rows, gain.shape[1]), jnp.bfloat16),
        in_specs=smem_specs(1) + vmem_specs(NY + 2),
        out_specs=pl.BlockSpec(memory_space=pltpu.VMEM),
        compiler_params=pltpu.CompilerParams(vmem_limit_bytes=10 * MB),
        cost_estimate=pl.CostEstimate(flops=2 * 10**9, bytes_accessed=6 * MB, transcendentals=0),
        name="normalise",
    )(order, *parts, rest, gain)


def up_kernel(start, left_ref, w_ref, out_ref):
    width = out_ref.shape[1]

    def step(n, carry):
        here = pl.ds(pl.multiple_of(n * 256, 256), 256)
        out_ref[here, :] = jnp.dot(
            left_ref[here, :], w_ref[:, start : start + width], preferred_element_type=jnp.float32
        ).astype(jnp.bfloat16)
        return carry

    lax.fori_loop(0, left_ref.shape[0] // 256, step, 0)


def up(left, weights, start, width):
    return pl.pallas_call(
        functools.partial(up_kernel, start),
        out_shape=jax.ShapeDtypeStruct((left.shape[0], width), jnp.bfloat16),
        in_specs=vmem_specs(2),
        out_specs=pl.BlockSpec(memory_space=pltpu.VMEM),
        compiler_params=pltpu.CompilerParams(vmem_limit_bytes=14 * MB),
        cost_estimate=pl.CostEstimate(flops=3 * 10**9, bytes_accessed=8 * MB, transcendentals=0),
    )(left, weights)


def hidden_kernel(value_ref, gate_ref, same_ref, before_ref, behind_ref, taps_ref, out_ref):
    rows, ff = out_ref.shape
    tail = gate_ref.shape[1]
    width = value_ref.shape[1]
    chunk = 256
    count = rows // chunk
    row = lax.broadcasted_iota(jnp.int32, (chunk, 128), 0)

    for at in range(0, width, 128):
        cols = slice(at, at + 128)
        if at < tail:
            low, high = before_ref[:, cols], behind_ref[:, cols]
            taps = taps_ref[:, cols].astype(jnp.float32)
        else:
            pad = ((0, 0), (0, at + 128 - ff))
            low, high = jnp.pad(before_ref[:, at:ff], pad), jnp.pad(behind_ref[:, at:ff], pad)
            taps = jnp.pad(taps_ref[:, at:ff].astype(jnp.float32), pad)
        low, high = low.astype(jnp.float32), high.astype(jnp.float32)

        def step(n, above):
            base = pl.multiple_of(n * chunk, chunk)
            here = pl.ds(base, chunk)
            value = value_ref[here, cols].astype(jnp.float32)
            following = pl.ds(pl.multiple_of(jnp.minimum(base + chunk, rows - 16), 16), 16)
            below = value_ref[following, cols].astype(jnp.float32)[:1]
            below = jnp.where(n == count - 1, high, below)
            prior = jnp.where(row == 0, above, pltpu.roll(value, 1, 0))
            after_ = jnp.where(row == chunk - 1, below, pltpu.roll(value, chunk - 1, 0))
            prev_same, next_same = same_ref[here, :1] > 0.5, same_ref[here, 1:2] > 0.5
            conv = (
                taps[0:1] * jnp.where(prev_same, prior, 0.0)
                + taps[1:2] * value
                + taps[2:3] * jnp.where(next_same, after_, 0.0)
            )
            act = conv * lax.logistic(conv)
            if at < tail:
                out_ref[here, cols] = (act * gate_ref[here, cols].astype(jnp.float32)).astype(
                    jnp.bfloat16
                )
            else:
                gate = pltpu.roll(value, 64, 1)
                out_ref[here, at:ff] = (act * gate).astype(jnp.bfloat16)[:, : ff - at]
            return value[chunk - 1 :]

        lax.fori_loop(0, count, step, low)


def hidden_units(value, gate, same, before, behind, taps):
    rows, ff = value.shape[0], taps.shape[1]
    return pl.pallas_call(
        hidden_kernel,
        out_shape=jax.ShapeDtypeStruct((rows, ff), jnp.bfloat16),
        in_specs=vmem_specs(6),
        out_specs=pl.BlockSpec(memory_space=pltpu.VMEM),
        compiler_params=pltpu.CompilerParams(vmem_limit_bytes=8 * MB),
        cost_estimate=pl.CostEstimate(flops=2 * 10**9, bytes_accessed=4 * MB, transcendentals=0),
        name="hidden_units",
    )(value, gate, same, before, behind, taps)


def to_owners(pairs):
    got = []
    for k in range(1, NY):
        got.append(lax.ppermute(pairs[k], "y", [(y, (y + k) % NY) for y in range(NY)]))
    return got


def per_device(
    queries,
    key_rows,
    values,
    sink_logits,
    doc_ids,
    residual,
    w_out,
    norm_gain,
    w_value_up,
    w_gate_up,
    conv_taps,
    w_down_t,
):
    model_width = residual.shape[1]
    span = model_width // (NY * NC)
    ff = w_value_up.shape[1]
    z, x, y, core = (lax.axis_index(axis) for axis in AXES)
    tp = y * NC + core
    order = jnp.stack(
        [((y + k) % NY) * NC + who for who in (core, 1 - core) for k in range(NY)]
        + [((y - k) % NY) * NC + who for who in (core, 1 - core) for k in range(NY)]
    )
    count = NZ * NX
    forward = [(i, i + 1) for i in range(count - 1)]
    backward = [(target, source) for source, target in forward]

    keys_t, vals_t = key_rows.T, values.T
    labels = (doc_ids + 1).astype(jnp.float32)[None, :]
    packed = jnp.concatenate([keys_t, vals_t, labels.astype(jnp.bfloat16)], axis=0)
    low = lax.ppermute(packed[:, -WINDOW:], ("z", "x"), forward)
    high = lax.ppermute(packed[:, :WINDOW], ("z", "x"), backward)

    tail = ff - ff % 128
    first = after(w_value_up, packed)
    share = jnp.concatenate(
        [w_gate_up[:, :tail], first, w_gate_up[:, tail:]], axis=1
    )
    rows_w, width = share.shape
    up_rows = lax.all_gather(share, "x", axis=0, tiled=True)

    def ring_step(plus, minus):
        plus = send_z(plus, 1)
        minus = send_z(minus, -1)
        return plus, minus

    def keep(full, plus, minus, k):
        return put(put(full, plus, (z - k) % NZ), minus, (z + k) % NZ)

    plus1, minus1 = ring_step(up_rows, up_rows)

    theirs, mine = attention(order, sink_logits, queries, packed, low, high, w_out)
    got = swap(theirs)

    pairs = pair_sums(mine, got)
    sent = to_owners(pairs)

    down1 = after(w_down_t, pairs[0])
    near = ring_step(down1, down1)
    far_plus = send_z(down1, 2)
    far_minus = send_z(down1, -2)

    plus2, minus2 = ring_step(plus1, minus1)
    third = ring_step(far_plus, far_minus)
    last = send_apart(jnp.where(core == 0, far_plus, far_minus), 2, 0)
    last_down = last

    own_res = lax.dynamic_slice_in_dim(residual, tp * span, span, 1)
    total = own_res.astype(jnp.float32)
    summed = pairs[0].astype(jnp.float32)
    for block in sent:
        summed = summed + block.astype(jnp.float32)
    mixed_own = (total + summed).astype(jnp.bfloat16)

    came = to_owners([mixed_own] * NY)
    came = lax.optimization_barrier((*came, plus2, minus2))[: NY - 1]
    parts = [mixed_own, *came]
    plus3, minus3 = ring_step(plus2, minus2)
    full = put(jnp.zeros((NZ,) + up_rows.shape, share.dtype), after(up_rows, mixed_own), z)
    full = keep(full, plus1, minus1, 1)
    whole = jnp.zeros((NZ,) + w_down_t.shape, w_down_t.dtype)
    whole = put(whole, after(w_down_t, mixed_own), z)
    whole = keep(whole, *near, 1)
    whole = keep(whole, far_plus, far_minus, 2)
    whole = keep(whole, *third, 3)
    whole = put(whole, last_down, (z + NZ // 2) % NZ)
    whole_plus = send_x(whole, 1)
    whole_minus = send_x(whole, -1)

    stacked = jnp.stack(parts)
    rest = swap(stacked)
    last = send_apart(jnp.where(core == 0, plus3, minus3), 1, 0)
    normed = normalised(order, parts, rest, norm_gain[None])
    full = keep(after(full, normed), plus2, minus2, 2)
    full = keep(full, plus3, minus3, 3)
    full = put(full, last, (z + NZ // 2) % NZ).reshape(model_width, width)

    whole_plus, whole_minus = lax.optimization_barrier((whole_plus, whole_minus, normed))[:2]
    whole_far = send_apart(jnp.where(core == 0, whole_plus, whole_minus), 0, 1)
    full_down = jnp.zeros((NZ, NX, rows_w, ff), w_down_t.dtype)
    full_down = put(full_down, after(whole, normed)[:, None], 0, x)
    full_down = put(full_down, whole_plus[:, None], 0, (x - 1) % NX)
    full_down = put(full_down, whole_minus[:, None], 0, (x + 1) % NX)
    full_down = put(full_down, whole_far[:, None], 0, (x + 2) % NX).reshape(model_width, ff)

    up_value = up(normed, full, tail, width - tail)
    before = lax.ppermute(up_value[-1:, :ff], ("z", "x"), forward)
    behind = lax.ppermute(up_value[:1, :ff], ("z", "x"), backward)
    up_gate = up(normed, full, 0, tail)
    low, packed, high = lax.optimization_barrier((low, packed, high, pairs[0]))[:3]
    edge = jnp.concatenate([low[-1:, -1:], packed[-1:], high[-1:, :1]], axis=1)[0]
    same = jnp.stack([edge[:-2] == edge[1:-1], edge[2:] == edge[1:-1]], axis=1)
    same = same.astype(jnp.float32)
    hidden = hidden_units(up_value, up_gate, same, before, behind, conv_taps)

    def down(who):
        weights = jnp.concatenate(
            [
                lax.dynamic_slice(
                    full_down, ((((y + k) % NY) * NC + who) * span, 0), (span, ff)
                )
                for k in range(NY)
            ],
            axis=0,
        )
        return lax.dot_general(
            hidden, weights, (((1,), (1,)), ((), ())), preferred_element_type=jnp.float32
        )

    got = swap(down(1 - core).astype(jnp.bfloat16))
    pair = (down(core) + got.astype(jnp.float32)).astype(jnp.bfloat16)
    pairs = [pair[:, k * span : (k + 1) * span] for k in range(NY)]
    ffn_cols = pairs[0].astype(jnp.float32)
    for block in to_owners(pairs):
        ffn_cols = ffn_cols + block.astype(jnp.float32)
    return (mixed_own.astype(jnp.float32) + ffn_cols).astype(jnp.bfloat16)


def solution(mesh):
    grid = Mesh(mesh.devices.reshape(NZ, NX, NY, NC), AXES)
    sp, tp = ("z", "x"), ("y", "core")
    placed = (
        P(sp, tp),
        P(sp, tp),
        P(sp, tp),
        P(tp),
        P(sp),
        P(sp, None),
        P(tp, None),
        P(),
        P(sp, tp),
        P(sp, tp),
        P(None, tp),
        P(sp, tp),
    )
    return jax.shard_map(
        per_device, mesh=grid, in_specs=placed, out_specs=P(sp, tp), check_vma=False
    )
```

```python
import functools

import jax
import jax.numpy as jnp
from jax import lax
from jax.experimental import pallas as pl
from jax.experimental.pallas import tpu as pltpu
from jax.sharding import Mesh
from jax.sharding import PartitionSpec as P

HEAD_DIM = 64
WINDOW = 128
EPS = 1e-06
NEG = -1e30

NZ, NX, NY, NC = 8, 4, 4, 2
AXES = ("z", "x", "y", "core")
MB = 1 << 20


def index_of(z, x, y, c):
    return (((z % NZ) * NX + x % NX) * NY + y % NY) * NC + c


def send_apart(block, dz, dx):
    pairs = [
        (index_of(z, x, y, c), index_of(z + s * dz, x + s * dx, y, c))
        for z in range(NZ)
        for x in range(NX)
        for y in range(NY)
        for c, s in ((0, 1), (1, -1))
    ]
    return lax.ppermute(block, AXES, pairs)


def send_z(block, k):
    return lax.ppermute(block, "z", [(z, (z + k) % NZ) for z in range(NZ)])


def send_x(block, k):
    return lax.ppermute(block, "x", [(x, (x + k) % NX) for x in range(NX)])


def swap(block):
    return lax.ppermute(block, "core", [(0, 1), (1, 0)])


def after(value, *others):
    return lax.optimization_barrier((value,) + others)[0]


def put(block, piece, *at):
    piece = piece.reshape((1,) * (block.ndim - piece.ndim) + piece.shape)
    start = list(at) + [0] * (block.ndim - len(at))
    return lax.dynamic_update_slice(block, piece, start)


def attention_kernel(
    at_ref, sink_ref, q_ref, w_ref, packed_ref, low_ref, high_ref,
    theirs_ref, mine_ref, same_ref,
    att_ref, kx_ref, vx_ref, row_ref, col_ref,
):
    rows = q_ref.shape[0]
    heads = q_ref.shape[1] // HEAD_DIM
    span = theirs_ref.shape[2]
    kx_ref[...] = jnp.zeros_like(kx_ref)
    vx_ref[...] = jnp.zeros_like(vx_ref)
    pieces = (
        (0, WINDOW, low_ref[:HEAD_DIM], low_ref[HEAD_DIM : 2 * HEAD_DIM]),
        (WINDOW, rows, packed_ref[:HEAD_DIM], packed_ref[HEAD_DIM : 2 * HEAD_DIM]),
        (WINDOW + rows, WINDOW, high_ref[:HEAD_DIM], high_ref[HEAD_DIM : 2 * HEAD_DIM]),
    )
    for start, width, keys, vals in pieces:
        vals_t = vals.astype(jnp.float32).T.astype(jnp.bfloat16)
        for h in range(heads):
            kx_ref[h, h * HEAD_DIM : (h + 1) * HEAD_DIM, start : start + width] = keys
            vx_ref[h, start : start + width, h * HEAD_DIM : (h + 1) * HEAD_DIM] = vals_t
    row_ref[:, :WINDOW] = jnp.broadcast_to(
        low_ref[2 * HEAD_DIM :].astype(jnp.float32), (8, WINDOW)
    )
    row_ref[:, WINDOW : WINDOW + rows] = jnp.broadcast_to(
        packed_ref[2 * HEAD_DIM :].astype(jnp.float32), (8, rows)
    )
    row_ref[:, WINDOW + rows :] = jnp.broadcast_to(
        high_ref[2 * HEAD_DIM :].astype(jnp.float32), (8, WINDOW)
    )
    for n in range(rows // WINDOW):
        part = row_ref[:, (n + 1) * WINDOW : (n + 2) * WINDOW]
        col_ref[n * WINDOW : (n + 1) * WINDOW, :] = jnp.broadcast_to(
            part[:1], (WINDOW, WINDOW)
        ).T

    label = col_ref[...]
    at_row = lax.broadcasted_iota(jnp.int32, (rows, WINDOW), 0)
    at_lane = lax.broadcasted_iota(jnp.int32, (rows, WINDOW), 1)
    first, last = row_ref[:1, WINDOW - 1 : WINDOW], row_ref[:1, WINDOW + rows : WINDOW + rows + 1]
    prior = jnp.where(at_row == 0, first, pltpu.roll(label, 1, 0))
    following = jnp.where(at_row == rows - 1, last, pltpu.roll(label, rows - 1, 0))
    other = jnp.where(at_lane == 0, prior, following)
    same_ref[...] = jnp.where(other == label, 1.0, 0.0)

    def step(n, carry):
        base = pl.multiple_of(n * WINDOW, WINDOW)
        here = pl.ds(base, WINDOW)
        window = pl.ds(base, 3 * WINDOW)
        q = q_ref[here, :] * jnp.bfloat16(HEAD_DIM ** (-0.5))
        offsets = (
            lax.broadcasted_iota(jnp.int32, (WINDOW, 3 * WINDOW), 1)
            - WINDOW
            - lax.broadcasted_iota(jnp.int32, (WINDOW, 3 * WINDOW), 0)
        )
        mine = col_ref[here, :1]
        allowed = (jnp.abs(offsets) <= WINDOW) & (row_ref[:1, window] == mine)
        acc = None
        for h in range(heads):
            score = jnp.dot(q, kx_ref[h, :, window], preferred_element_type=jnp.float32)
            score = jnp.where(allowed, score, NEG)
            highest = jnp.maximum(jnp.max(score, axis=1, keepdims=True), sink_ref[h])
            raw = jnp.exp(score - highest)
            total = jnp.sum(raw, axis=1, keepdims=True) + jnp.exp(sink_ref[h] - highest)
            probs = (raw * (1.0 / total)).astype(jnp.bfloat16)
            part = jnp.dot(probs, vx_ref[h, window, :], preferred_element_type=jnp.float32)
            acc = part if acc is None else acc + part
        att_ref[here, :] = acc.astype(jnp.bfloat16)
        return carry

    lax.fori_loop(0, rows // WINDOW, step, 0)
    for k in range(NY):
        cols = pl.ds(pl.multiple_of(at_ref[NY + k] * span, span), span)
        theirs_ref[k] = jnp.dot(
            att_ref[...], w_ref[:, cols], preferred_element_type=jnp.float32
        ).astype(jnp.bfloat16)
        cols = pl.ds(pl.multiple_of(at_ref[k] * span, span), span)
        mine_ref[k] = jnp.dot(
            att_ref[...], w_ref[:, cols], preferred_element_type=jnp.float32
        ).astype(jnp.bfloat16)


def vmem_specs(count):
    return [pl.BlockSpec(memory_space=pltpu.VMEM)] * count


def smem_specs(count):
    return [pl.BlockSpec(memory_space=pltpu.SMEM)] * count


def attention(order, sink, queries, packed, low, high, w_out):
    rows, cols = queries.shape
    span = w_out.shape[1] // (NY * NC)
    reach = rows + 2 * WINDOW
    heads = cols // HEAD_DIM
    return pl.pallas_call(
        attention_kernel,
        out_shape=[
            jax.ShapeDtypeStruct((NY, rows, span), jnp.bfloat16),
            jax.ShapeDtypeStruct((NY, rows, span), jnp.bfloat16),
            jax.ShapeDtypeStruct((rows, WINDOW), jnp.float32),
        ],
        in_specs=smem_specs(2) + vmem_specs(5),
        out_specs=vmem_specs(3),
        scratch_shapes=[
            pltpu.VMEM((rows, cols), jnp.bfloat16),
            pltpu.VMEM((heads, cols, reach), jnp.bfloat16),
            pltpu.VMEM((heads, reach, cols), jnp.bfloat16),
            pltpu.VMEM((8, reach), jnp.float32),
            pltpu.VMEM((rows, WINDOW), jnp.float32),
        ],
        compiler_params=pltpu.CompilerParams(vmem_limit_bytes=12 * MB),
        cost_estimate=pl.CostEstimate(flops=4 * 10**9, bytes_accessed=4 * MB, transcendentals=0),
        name="attention",
    )(order, sink, queries, w_out, packed, low, high)


def pair_kernel(mine_ref, got_ref, s0, s1, s2, s3):
    for k, out in enumerate((s0, s1, s2, s3)):
        out[...] = (
            mine_ref[k].astype(jnp.float32) + got_ref[k].astype(jnp.float32)
        ).astype(jnp.bfloat16)


def pair_sums(mine, got):
    return pl.pallas_call(
        pair_kernel,
        out_shape=[jax.ShapeDtypeStruct(got.shape[1:], jnp.bfloat16)] * NY,
        in_specs=vmem_specs(2),
        out_specs=vmem_specs(NY),
        compiler_params=pltpu.CompilerParams(vmem_limit_bytes=8 * MB),
        cost_estimate=pl.CostEstimate(flops=10**9, bytes_accessed=4 * MB, transcendentals=0),
        name="pair_sums",
    )(mine, got)


def norm_kernel(at_ref, p0, p1, p2, p3, rest_ref, gain_ref, out_ref):
    rows, span = p0.shape
    width = out_ref.shape[1]

    def step(n, carry):
        here = pl.ds(pl.multiple_of(n * 64, 64), 64)
        mine = [ref[here, :].astype(jnp.float32) for ref in (p0, p1, p2, p3)]
        theirs = [rest_ref[k, here, :].astype(jnp.float32) for k in range(NY)]
        square = sum(block * block for block in mine + theirs)
        mean_sq = jnp.sum(square, axis=1, keepdims=True) * (1.0 / width)
        scale = lax.rsqrt(mean_sq + EPS)
        for k, block in enumerate(mine + theirs):
            cols = pl.ds(pl.multiple_of(at_ref[2 * NY + k] * span, span), span)
            out_ref[here, cols] = (block * scale * gain_ref[:, cols]).astype(jnp.bfloat16)
        return carry

    lax.fori_loop(0, rows // 64, step, 0)


def normalised(order, parts, rest, gain):
    rows, _ = parts[0].shape
    return pl.pallas_call(
        norm_kernel,
        out_shape=jax.ShapeDtypeStruct((rows, gain.shape[1]), jnp.bfloat16),
        in_specs=smem_specs(1) + vmem_specs(NY + 2),
        out_specs=pl.BlockSpec(memory_space=pltpu.VMEM),
        compiler_params=pltpu.CompilerParams(vmem_limit_bytes=10 * MB),
        cost_estimate=pl.CostEstimate(flops=2 * 10**9, bytes_accessed=6 * MB, transcendentals=0),
        name="normalise",
    )(order, *parts, rest, gain)


def up_kernel(start, left_ref, w_ref, out_ref):
    width = out_ref.shape[1]

    def step(n, carry):
        here = pl.ds(pl.multiple_of(n * 256, 256), 256)
        out_ref[here, :] = jnp.dot(
            left_ref[here, :], w_ref[:, start : start + width], preferred_element_type=jnp.float32
        ).astype(jnp.bfloat16)
        return carry

    lax.fori_loop(0, left_ref.shape[0] // 256, step, 0)


def up(left, weights, start, width):
    return pl.pallas_call(
        functools.partial(up_kernel, start),
        out_shape=jax.ShapeDtypeStruct((left.shape[0], width), jnp.bfloat16),
        in_specs=vmem_specs(2),
        out_specs=pl.BlockSpec(memory_space=pltpu.VMEM),
        compiler_params=pltpu.CompilerParams(vmem_limit_bytes=14 * MB),
        cost_estimate=pl.CostEstimate(flops=3 * 10**9, bytes_accessed=8 * MB, transcendentals=0),
    )(left, weights)


def hidden_kernel(value_ref, gate_ref, same_ref, before_ref, behind_ref, taps_ref, out_ref):
    rows, ff = out_ref.shape
    tail = gate_ref.shape[1]
    width = value_ref.shape[1]
    chunk = 256
    count = rows // chunk
    row = lax.broadcasted_iota(jnp.int32, (chunk, 128), 0)

    for at in range(0, width, 128):
        cols = slice(at, at + 128)
        if at < tail:
            low, high = before_ref[:, cols], behind_ref[:, cols]
            taps = taps_ref[:, cols].astype(jnp.float32)
        else:
            pad = ((0, 0), (0, at + 128 - ff))
            low, high = jnp.pad(before_ref[:, at:ff], pad), jnp.pad(behind_ref[:, at:ff], pad)
            taps = jnp.pad(taps_ref[:, at:ff].astype(jnp.float32), pad)
        low, high = low.astype(jnp.float32), high.astype(jnp.float32)

        def step(n, above):
            base = pl.multiple_of(n * chunk, chunk)
            here = pl.ds(base, chunk)
            value = value_ref[here, cols].astype(jnp.float32)
            following = pl.ds(pl.multiple_of(jnp.minimum(base + chunk, rows - 16), 16), 16)
            below = value_ref[following, cols].astype(jnp.float32)[:1]
            below = jnp.where(n == count - 1, high, below)
            prior = jnp.where(row == 0, above, pltpu.roll(value, 1, 0))
            after_ = jnp.where(row == chunk - 1, below, pltpu.roll(value, chunk - 1, 0))
            prev_same, next_same = same_ref[here, :1] > 0.5, same_ref[here, 1:2] > 0.5
            conv = (
                taps[0:1] * jnp.where(prev_same, prior, 0.0)
                + taps[1:2] * value
                + taps[2:3] * jnp.where(next_same, after_, 0.0)
            )
            act = conv * lax.logistic(conv)
            if at < tail:
                out_ref[here, cols] = (act * gate_ref[here, cols].astype(jnp.float32)).astype(
                    jnp.bfloat16
                )
            else:
                gate = pltpu.roll(value, 64, 1)
                out_ref[here, at:ff] = (act * gate).astype(jnp.bfloat16)[:, : ff - at]
            return value[chunk - 1 :]

        lax.fori_loop(0, count, step, low)


def hidden_units(value, gate, same, before, behind, taps):
    rows, ff = value.shape[0], taps.shape[1]
    return pl.pallas_call(
        hidden_kernel,
        out_shape=jax.ShapeDtypeStruct((rows, ff), jnp.bfloat16),
        in_specs=vmem_specs(6),
        out_specs=pl.BlockSpec(memory_space=pltpu.VMEM),
        compiler_params=pltpu.CompilerParams(vmem_limit_bytes=8 * MB),
        cost_estimate=pl.CostEstimate(flops=2 * 10**9, bytes_accessed=4 * MB, transcendentals=0),
        name="hidden_units",
    )(value, gate, same, before, behind, taps)


def to_owners(pairs):
    got = []
    for k in range(1, NY):
        got.append(lax.ppermute(pairs[k], "y", [(y, (y + k) % NY) for y in range(NY)]))
    return got


def per_device(
    queries,
    key_rows,
    values,
    sink_logits,
    doc_ids,
    residual,
    w_out,
    norm_gain,
    w_value_up,
    w_gate_up,
    conv_taps,
    w_down_t,
):
    model_width = residual.shape[1]
    span = model_width // (NY * NC)
    ff = w_value_up.shape[1]
    z, x, y, core = (lax.axis_index(axis) for axis in AXES)
    tp = y * NC + core
    order = jnp.stack(
        [((y + k) % NY) * NC + who for who in (core, 1 - core) for k in range(NY)]
        + [((y - k) % NY) * NC + who for who in (core, 1 - core) for k in range(NY)]
    )
    count = NZ * NX
    forward = [(i, i + 1) for i in range(count - 1)]
    backward = [(target, source) for source, target in forward]

    keys_t, vals_t = key_rows.T, values.T
    labels = (doc_ids + 1).astype(jnp.float32)[None, :]
    packed = jnp.concatenate([keys_t, vals_t, labels.astype(jnp.bfloat16)], axis=0)
    low = lax.ppermute(packed[:, -WINDOW:], ("z", "x"), forward)
    high = lax.ppermute(packed[:, :WINDOW], ("z", "x"), backward)

    tail = ff - ff % 128
    first = after(w_value_up, packed)
    share = jnp.concatenate(
        [w_gate_up[:, :tail], first, w_gate_up[:, tail:]], axis=1
    )
    rows_w, width = share.shape
    up_rows = lax.all_gather(share, "x", axis=0, tiled=True)

    def ring_step(plus, minus):
        plus = send_z(plus, 1)
        minus = send_z(minus, -1)
        return plus, minus

    def keep(full, plus, minus, k):
        return put(put(full, plus, (z - k) % NZ), minus, (z + k) % NZ)

    plus1, minus1 = ring_step(up_rows, up_rows)

    theirs, mine, same = attention(order, sink_logits, queries, packed, low, high, w_out)
    got = swap(theirs)

    pairs = pair_sums(mine, got)
    sent = to_owners(pairs)

    down1 = after(w_down_t, pairs[0])
    near = ring_step(down1, down1)
    far_plus = send_z(down1, 2)
    far_minus = send_z(down1, -2)

    plus2, minus2 = ring_step(plus1, minus1)
    third = ring_step(far_plus, far_minus)
    last = send_apart(jnp.where(core == 0, far_plus, far_minus), 2, 0)
    last_down = last

    own_res = lax.dynamic_slice_in_dim(residual, tp * span, span, 1)
    total = own_res.astype(jnp.float32)
    summed = pairs[0].astype(jnp.float32)
    for block in sent:
        summed = summed + block.astype(jnp.float32)
    mixed_own = (total + summed).astype(jnp.bfloat16)

    came = to_owners([mixed_own] * NY)
    came = lax.optimization_barrier((*came, plus2, minus2))[: NY - 1]
    parts = [mixed_own, *came]
    plus3, minus3 = ring_step(plus2, minus2)
    full = put(jnp.zeros((NZ,) + up_rows.shape, share.dtype), after(up_rows, mixed_own), z)
    full = keep(full, plus1, minus1, 1)
    whole = jnp.zeros((NZ,) + w_down_t.shape, w_down_t.dtype)
    whole = put(whole, after(w_down_t, mixed_own, plus2, minus2), z)
    whole = keep(whole, *near, 1)
    whole = keep(whole, far_plus, far_minus, 2)
    whole = keep(whole, *third, 3)
    whole = put(whole, last_down, (z + NZ // 2) % NZ)
    whole_plus = send_x(whole, 1)
    whole_minus = send_x(whole, -1)

    stacked = jnp.stack(parts)
    rest = swap(stacked)
    last = send_apart(jnp.where(core == 0, plus3, minus3), 1, 0)
    normed = normalised(order, parts, rest, norm_gain[None])
    full = keep(after(full, normed), plus2, minus2, 2)
    full = keep(full, plus3, minus3, 3)
    full = put(full, last, (z + NZ // 2) % NZ).reshape(model_width, width)

    whole_plus, whole_minus = lax.optimization_barrier((whole_plus, whole_minus, normed))[:2]
    whole_far = send_apart(jnp.where(core == 0, whole_plus, whole_minus), 0, 1)
    full_down = jnp.zeros((NZ, NX, rows_w, ff), w_down_t.dtype)
    full_down = put(full_down, after(whole, normed)[:, None], 0, x)
    full_down = put(full_down, whole_plus[:, None], 0, (x - 1) % NX)
    full_down = put(full_down, whole_minus[:, None], 0, (x + 1) % NX)
    normed = after(normed, full_down)
    full_down = put(full_down, whole_far[:, None], 0, (x + 2) % NX).reshape(model_width, ff)

    up_value = up(normed, full, tail, width - tail)
    before = lax.ppermute(up_value[-1:, :ff], ("z", "x"), forward)
    behind = lax.ppermute(up_value[:1, :ff], ("z", "x"), backward)
    up_gate = up(normed, full, 0, tail)
    hidden = hidden_units(up_value, up_gate, same, before, behind, conv_taps)

    def down(who):
        weights = jnp.concatenate(
            [
                lax.dynamic_slice(
                    full_down, ((((y + k) % NY) * NC + who) * span, 0), (span, ff)
                )
                for k in range(NY)
            ],
            axis=0,
        )
        return lax.dot_general(
            hidden, weights, (((1,), (1,)), ((), ())), preferred_element_type=jnp.float32
        )

    got = swap(down(1 - core).astype(jnp.bfloat16))
    pair = (down(core) + got.astype(jnp.float32)).astype(jnp.bfloat16)
    pairs = [pair[:, k * span : (k + 1) * span] for k in range(NY)]
    ffn_cols = pairs[0].astype(jnp.float32)
    for block in to_owners(pairs):
        ffn_cols = ffn_cols + block.astype(jnp.float32)
    return (mixed_own.astype(jnp.float32) + ffn_cols).astype(jnp.bfloat16)


def solution(mesh):
    grid = Mesh(mesh.devices.reshape(NZ, NX, NY, NC), AXES)
    sp, tp = ("z", "x"), ("y", "core")
    placed = (
        P(sp, tp),
        P(sp, tp),
        P(sp, tp),
        P(tp),
        P(sp),
        P(sp, None),
        P(tp, None),
        P(),
        P(sp, tp),
        P(sp, tp),
        P(None, tp),
        P(sp, tp),
    )
    return jax.shard_map(
        per_device, mesh=grid, in_specs=placed, out_specs=P(sp, tp), check_vma=False
    )
```

```python
import functools

import jax
import jax.numpy as jnp
from jax import lax
from jax.experimental import pallas as pl
from jax.experimental.pallas import tpu as pltpu
from jax.sharding import Mesh
from jax.sharding import PartitionSpec as P

HEAD_DIM = 64
WINDOW = 128
EPS = 1e-06
NEG = -1e30

NZ, NX, NY, NC = 8, 4, 4, 2
AXES = ("z", "x", "y", "core")
MB = 1 << 20


def index_of(z, x, y, c):
    return (((z % NZ) * NX + x % NX) * NY + y % NY) * NC + c


def send_apart(block, dz, dx):
    pairs = [
        (index_of(z, x, y, c), index_of(z + s * dz, x + s * dx, y, c))
        for z in range(NZ)
        for x in range(NX)
        for y in range(NY)
        for c, s in ((0, 1), (1, -1))
    ]
    return lax.ppermute(block, AXES, pairs)


def send_z(block, k):
    return lax.ppermute(block, "z", [(z, (z + k) % NZ) for z in range(NZ)])


def send_x(block, k):
    return lax.ppermute(block, "x", [(x, (x + k) % NX) for x in range(NX)])


def swap(block):
    return lax.ppermute(block, "core", [(0, 1), (1, 0)])


def after(value, *others):
    return lax.optimization_barrier((value,) + others)[0]


def put(block, piece, *at):
    piece = piece.reshape((1,) * (block.ndim - piece.ndim) + piece.shape)
    start = list(at) + [0] * (block.ndim - len(at))
    return lax.dynamic_update_slice(block, piece, start)


def attention_kernel(
    at_ref, sink_ref, q_ref, w_ref, packed_ref, low_ref, high_ref,
    theirs_ref, mine_ref, same_ref,
    att_ref, kx_ref, vx_ref, row_ref, col_ref,
):
    rows = q_ref.shape[0]
    heads = q_ref.shape[1] // HEAD_DIM
    span = theirs_ref.shape[2]
    kx_ref[...] = jnp.zeros_like(kx_ref)
    vx_ref[...] = jnp.zeros_like(vx_ref)
    pieces = (
        (0, WINDOW, low_ref[:HEAD_DIM], low_ref[HEAD_DIM : 2 * HEAD_DIM]),
        (WINDOW, rows, packed_ref[:HEAD_DIM], packed_ref[HEAD_DIM : 2 * HEAD_DIM]),
        (WINDOW + rows, WINDOW, high_ref[:HEAD_DIM], high_ref[HEAD_DIM : 2 * HEAD_DIM]),
    )
    for start, width, keys, vals in pieces:
        vals_t = vals.astype(jnp.float32).T.astype(jnp.bfloat16)
        for h in range(heads):
            kx_ref[h, h * HEAD_DIM : (h + 1) * HEAD_DIM, start : start + width] = keys
            vx_ref[h, start : start + width, h * HEAD_DIM : (h + 1) * HEAD_DIM] = vals_t
    row_ref[:, :WINDOW] = jnp.broadcast_to(
        low_ref[2 * HEAD_DIM :].astype(jnp.float32), (8, WINDOW)
    )
    row_ref[:, WINDOW : WINDOW + rows] = jnp.broadcast_to(
        packed_ref[2 * HEAD_DIM :].astype(jnp.float32), (8, rows)
    )
    row_ref[:, WINDOW + rows :] = jnp.broadcast_to(
        high_ref[2 * HEAD_DIM :].astype(jnp.float32), (8, WINDOW)
    )
    for n in range(rows // WINDOW):
        part = row_ref[:, (n + 1) * WINDOW : (n + 2) * WINDOW]
        col_ref[n * WINDOW : (n + 1) * WINDOW, :] = jnp.broadcast_to(
            part[:1], (WINDOW, WINDOW)
        ).T

    label = col_ref[...]
    at_row = lax.broadcasted_iota(jnp.int32, (rows, WINDOW), 0)
    at_lane = lax.broadcasted_iota(jnp.int32, (rows, WINDOW), 1)
    first, last = row_ref[:1, WINDOW - 1 : WINDOW], row_ref[:1, WINDOW + rows : WINDOW + rows + 1]
    prior = jnp.where(at_row == 0, first, pltpu.roll(label, 1, 0))
    following = jnp.where(at_row == rows - 1, last, pltpu.roll(label, rows - 1, 0))
    other = jnp.where(at_lane == 0, prior, following)
    same_ref[...] = jnp.where(other == label, 1.0, 0.0)

    def step(n, carry):
        base = pl.multiple_of(n * WINDOW, WINDOW)
        here = pl.ds(base, WINDOW)
        window = pl.ds(base, 3 * WINDOW)
        q = q_ref[here, :] * jnp.bfloat16(HEAD_DIM ** (-0.5))
        offsets = (
            lax.broadcasted_iota(jnp.int32, (WINDOW, 3 * WINDOW), 1)
            - WINDOW
            - lax.broadcasted_iota(jnp.int32, (WINDOW, 3 * WINDOW), 0)
        )
        mine = col_ref[here, :1]
        allowed = (jnp.abs(offsets) <= WINDOW) & (row_ref[:1, window] == mine)
        acc = None
        for h in range(heads):
            score = jnp.dot(q, kx_ref[h, :, window], preferred_element_type=jnp.float32)
            score = jnp.where(allowed, score, NEG)
            highest = jnp.maximum(jnp.max(score, axis=1, keepdims=True), sink_ref[h])
            raw = jnp.exp(score - highest)
            total = jnp.sum(raw, axis=1, keepdims=True) + jnp.exp(sink_ref[h] - highest)
            probs = (raw * (1.0 / total)).astype(jnp.bfloat16)
            part = jnp.dot(probs, vx_ref[h, window, :], preferred_element_type=jnp.float32)
            acc = part if acc is None else acc + part
        att_ref[here, :] = acc.astype(jnp.bfloat16)
        return carry

    lax.fori_loop(0, rows // WINDOW, step, 0)
    for k in range(NY):
        cols = pl.ds(pl.multiple_of(at_ref[NY + k] * span, span), span)
        theirs_ref[k] = jnp.dot(
            att_ref[...], w_ref[:, cols], preferred_element_type=jnp.float32
        ).astype(jnp.bfloat16)
        cols = pl.ds(pl.multiple_of(at_ref[k] * span, span), span)
        mine_ref[k] = jnp.dot(
            att_ref[...], w_ref[:, cols], preferred_element_type=jnp.float32
        ).astype(jnp.bfloat16)


def vmem_specs(count):
    return [pl.BlockSpec(memory_space=pltpu.VMEM)] * count


def smem_specs(count):
    return [pl.BlockSpec(memory_space=pltpu.SMEM)] * count


def attention(order, sink, queries, packed, low, high, w_out):
    rows, cols = queries.shape
    span = w_out.shape[1] // (NY * NC)
    reach = rows + 2 * WINDOW
    heads = cols // HEAD_DIM
    return pl.pallas_call(
        attention_kernel,
        out_shape=[
            jax.ShapeDtypeStruct((NY, rows, span), jnp.bfloat16),
            jax.ShapeDtypeStruct((NY, rows, span), jnp.bfloat16),
            jax.ShapeDtypeStruct((rows, WINDOW), jnp.float32),
        ],
        in_specs=smem_specs(2) + vmem_specs(5),
        out_specs=vmem_specs(3),
        scratch_shapes=[
            pltpu.VMEM((rows, cols), jnp.bfloat16),
            pltpu.VMEM((heads, cols, reach), jnp.bfloat16),
            pltpu.VMEM((heads, reach, cols), jnp.bfloat16),
            pltpu.VMEM((8, reach), jnp.float32),
            pltpu.VMEM((rows, WINDOW), jnp.float32),
        ],
        compiler_params=pltpu.CompilerParams(vmem_limit_bytes=12 * MB),
        cost_estimate=pl.CostEstimate(flops=4 * 10**9, bytes_accessed=4 * MB, transcendentals=0),
        name="attention",
    )(order, sink, queries, w_out, packed, low, high)


def pair_kernel(mine_ref, got_ref, s0, s1, s2, s3):
    for k, out in enumerate((s0, s1, s2, s3)):
        out[...] = (
            mine_ref[k].astype(jnp.float32) + got_ref[k].astype(jnp.float32)
        ).astype(jnp.bfloat16)


def pair_sums(mine, got):
    return pl.pallas_call(
        pair_kernel,
        out_shape=[jax.ShapeDtypeStruct(got.shape[1:], jnp.bfloat16)] * NY,
        in_specs=vmem_specs(2),
        out_specs=vmem_specs(NY),
        compiler_params=pltpu.CompilerParams(vmem_limit_bytes=8 * MB),
        cost_estimate=pl.CostEstimate(flops=10**9, bytes_accessed=4 * MB, transcendentals=0),
        name="pair_sums",
    )(mine, got)


def norm_kernel(at_ref, p0, p1, p2, p3, rest_ref, gain_ref, out_ref):
    rows, span = p0.shape
    width = out_ref.shape[1]

    def step(n, carry):
        here = pl.ds(pl.multiple_of(n * 64, 64), 64)
        mine = [ref[here, :].astype(jnp.float32) for ref in (p0, p1, p2, p3)]
        theirs = [rest_ref[k, here, :].astype(jnp.float32) for k in range(NY)]
        square = sum(block * block for block in mine + theirs)
        mean_sq = jnp.sum(square, axis=1, keepdims=True) * (1.0 / width)
        scale = lax.rsqrt(mean_sq + EPS)
        for k, block in enumerate(mine + theirs):
            cols = pl.ds(pl.multiple_of(at_ref[2 * NY + k] * span, span), span)
            out_ref[here, cols] = (block * scale * gain_ref[:, cols]).astype(jnp.bfloat16)
        return carry

    lax.fori_loop(0, rows // 64, step, 0)


def normalised(order, parts, rest, gain):
    rows, _ = parts[0].shape
    return pl.pallas_call(
        norm_kernel,
        out_shape=jax.ShapeDtypeStruct((rows, gain.shape[1]), jnp.bfloat16),
        in_specs=smem_specs(1) + vmem_specs(NY + 2),
        out_specs=pl.BlockSpec(memory_space=pltpu.VMEM),
        compiler_params=pltpu.CompilerParams(vmem_limit_bytes=10 * MB),
        cost_estimate=pl.CostEstimate(flops=2 * 10**9, bytes_accessed=6 * MB, transcendentals=0),
        name="normalise",
    )(order, *parts, rest, gain)


def up_kernel(start, left_ref, w_ref, out_ref):
    width = out_ref.shape[1]

    def step(n, carry):
        here = pl.ds(pl.multiple_of(n * 256, 256), 256)
        out_ref[here, :] = jnp.dot(
            left_ref[here, :], w_ref[:, start : start + width], preferred_element_type=jnp.float32
        ).astype(jnp.bfloat16)
        return carry

    lax.fori_loop(0, left_ref.shape[0] // 256, step, 0)


def up(left, weights, start, width):
    return pl.pallas_call(
        functools.partial(up_kernel, start),
        out_shape=jax.ShapeDtypeStruct((left.shape[0], width), jnp.bfloat16),
        in_specs=vmem_specs(2),
        out_specs=pl.BlockSpec(memory_space=pltpu.VMEM),
        compiler_params=pltpu.CompilerParams(vmem_limit_bytes=14 * MB),
        cost_estimate=pl.CostEstimate(flops=3 * 10**9, bytes_accessed=8 * MB, transcendentals=0),
    )(left, weights)


def hidden_kernel(value_ref, gate_ref, same_ref, before_ref, behind_ref, taps_ref, out_ref):
    rows, ff = out_ref.shape
    tail = gate_ref.shape[1]
    width = value_ref.shape[1]
    chunk = 256
    count = rows // chunk
    row = lax.broadcasted_iota(jnp.int32, (chunk, 128), 0)

    for at in range(0, width, 128):
        cols = slice(at, at + 128)
        if at < tail:
            low, high = before_ref[:, cols], behind_ref[:, cols]
            taps = taps_ref[:, cols].astype(jnp.float32)
        else:
            pad = ((0, 0), (0, at + 128 - ff))
            low, high = jnp.pad(before_ref[:, at:ff], pad), jnp.pad(behind_ref[:, at:ff], pad)
            taps = jnp.pad(taps_ref[:, at:ff].astype(jnp.float32), pad)
        low, high = low.astype(jnp.float32), high.astype(jnp.float32)

        def step(n, above):
            base = pl.multiple_of(n * chunk, chunk)
            here = pl.ds(base, chunk)
            value = value_ref[here, cols].astype(jnp.float32)
            following = pl.ds(pl.multiple_of(jnp.minimum(base + chunk, rows - 16), 16), 16)
            below = value_ref[following, cols].astype(jnp.float32)[:1]
            below = jnp.where(n == count - 1, high, below)
            prior = jnp.where(row == 0, above, pltpu.roll(value, 1, 0))
            after_ = jnp.where(row == chunk - 1, below, pltpu.roll(value, chunk - 1, 0))
            prev_same, next_same = same_ref[here, :1] > 0.5, same_ref[here, 1:2] > 0.5
            conv = (
                taps[0:1] * jnp.where(prev_same, prior, 0.0)
                + taps[1:2] * value
                + taps[2:3] * jnp.where(next_same, after_, 0.0)
            )
            act = conv * lax.logistic(conv)
            if at < tail:
                out_ref[here, cols] = (act * gate_ref[here, cols].astype(jnp.float32)).astype(
                    jnp.bfloat16
                )
            else:
                gate = pltpu.roll(value, 64, 1)
                out_ref[here, at:ff] = (act * gate).astype(jnp.bfloat16)[:, : ff - at]
            return value[chunk - 1 :]

        lax.fori_loop(0, count, step, low)


def hidden_units(value, gate, same, before, behind, taps):
    rows, ff = value.shape[0], taps.shape[1]
    return pl.pallas_call(
        hidden_kernel,
        out_shape=jax.ShapeDtypeStruct((rows, ff), jnp.bfloat16),
        in_specs=vmem_specs(6),
        out_specs=pl.BlockSpec(memory_space=pltpu.VMEM),
        compiler_params=pltpu.CompilerParams(vmem_limit_bytes=8 * MB),
        cost_estimate=pl.CostEstimate(flops=2 * 10**9, bytes_accessed=4 * MB, transcendentals=0),
        name="hidden_units",
    )(value, gate, same, before, behind, taps)


def to_owners(pairs):
    got = []
    for k in range(1, NY):
        got.append(lax.ppermute(pairs[k], "y", [(y, (y + k) % NY) for y in range(NY)]))
    return got


def per_device(
    queries,
    key_rows,
    values,
    sink_logits,
    doc_ids,
    residual,
    w_out,
    norm_gain,
    w_value_up,
    w_gate_up,
    conv_taps,
    w_down_t,
):
    model_width = residual.shape[1]
    span = model_width // (NY * NC)
    ff = w_value_up.shape[1]
    z, x, y, core = (lax.axis_index(axis) for axis in AXES)
    tp = y * NC + core
    order = jnp.stack(
        [((y + k) % NY) * NC + who for who in (core, 1 - core) for k in range(NY)]
        + [((y - k) % NY) * NC + who for who in (core, 1 - core) for k in range(NY)]
    )
    count = NZ * NX
    forward = [(i, i + 1) for i in range(count - 1)]
    backward = [(target, source) for source, target in forward]

    keys_t, vals_t = key_rows.T, values.T
    labels = (doc_ids + 1).astype(jnp.float32)[None, :]
    packed = jnp.concatenate([keys_t, vals_t, labels.astype(jnp.bfloat16)], axis=0)
    low = lax.ppermute(packed[:, -WINDOW:], ("z", "x"), forward)
    high = lax.ppermute(packed[:, :WINDOW], ("z", "x"), backward)

    tail = ff - ff % 128
    first = after(w_value_up, packed)
    share = jnp.concatenate(
        [w_gate_up[:, :tail], first, w_gate_up[:, tail:]], axis=1
    )
    rows_w, width = share.shape
    gathered = []
    for k in range(1, NX):
        gathered.append(send_x(share, k))

    def ring_step(plus, minus):
        plus = send_z(plus, 1)
        minus = send_z(minus, -1)
        return plus, minus

    def keep(full, plus, minus, k):
        return put(put(full, plus, (z - k) % NZ), minus, (z + k) % NZ)

    theirs, mine, same = attention(order, sink_logits, queries, packed, low, high, w_out)
    got = swap(theirs)

    gathered = lax.optimization_barrier((*gathered, theirs))[:-1]
    up_rows = put(jnp.zeros((NX, rows_w, width), share.dtype), share, x)
    for k, piece in enumerate(gathered):
        up_rows = put(up_rows, piece, (x - k - 1) % NX)
    up_rows = up_rows.reshape(NX * rows_w, width)
    plus1, minus1 = ring_step(up_rows, up_rows)

    pairs = pair_sums(mine, got)
    sent = to_owners(pairs)

    down1 = after(w_down_t, pairs[0])
    near = ring_step(down1, down1)
    far_plus = send_z(down1, 2)
    far_minus = send_z(down1, -2)

    plus2, minus2 = ring_step(plus1, minus1)
    own_res = lax.dynamic_slice_in_dim(residual, tp * span, span, 1)
    summed = pairs[0].astype(jnp.float32)
    for block in sent:
        summed = summed + block.astype(jnp.float32)
    mixed_own = (own_res.astype(jnp.float32) + summed).astype(jnp.bfloat16)

    far_plus, far_minus = lax.optimization_barrier((far_plus, far_minus, mixed_own))[:2]
    third = ring_step(far_plus, far_minus)
    last_down = send_apart(jnp.where(core == 0, far_plus, far_minus), 2, 0)

    came = to_owners([mixed_own] * NY)
    came = lax.optimization_barrier((*came, plus2, minus2))[: NY - 1]
    parts = [mixed_own, *came]
    plus3, minus3 = ring_step(plus2, minus2)
    full = put(jnp.zeros((NZ,) + up_rows.shape, share.dtype), after(up_rows, mixed_own), z)
    full = keep(full, plus1, minus1, 1)
    whole = jnp.zeros((NZ,) + w_down_t.shape, w_down_t.dtype)
    whole = put(whole, after(w_down_t, mixed_own, plus2, minus2), z)
    whole = keep(whole, *near, 1)
    whole = keep(whole, far_plus, far_minus, 2)
    whole = keep(whole, *third, 3)
    whole = put(whole, last_down, (z + NZ // 2) % NZ)
    whole_plus = send_x(whole, 1)
    whole_minus = send_x(whole, -1)

    stacked = jnp.stack(parts)
    rest = swap(stacked)
    last = send_apart(jnp.where(core == 0, plus3, minus3), 1, 0)
    normed = normalised(order, parts, rest, norm_gain[None])
    full = keep(after(full, normed), plus2, minus2, 2)
    full = keep(full, plus3, minus3, 3)
    full = put(full, last, (z + NZ // 2) % NZ).reshape(model_width, width)

    whole_plus, whole_minus = lax.optimization_barrier((whole_plus, whole_minus, normed))[:2]
    whole_far = send_apart(jnp.where(core == 0, whole_plus, whole_minus), 0, 1)
    full_down = jnp.zeros((NZ, NX, rows_w, ff), w_down_t.dtype)
    full_down = put(full_down, after(whole, normed)[:, None], 0, x)
    full_down = put(full_down, whole_plus[:, None], 0, (x - 1) % NX)
    full_down = put(full_down, whole_minus[:, None], 0, (x + 1) % NX)
    normed = after(normed, full_down)
    full_down = put(full_down, whole_far[:, None], 0, (x + 2) % NX).reshape(model_width, ff)

    up_value = up(normed, full, tail, width - tail)
    before = lax.ppermute(up_value[-1:, :ff], ("z", "x"), forward)
    behind = lax.ppermute(up_value[:1, :ff], ("z", "x"), backward)
    up_gate = up(normed, full, 0, tail)
    hidden = hidden_units(up_value, up_gate, same, before, behind, conv_taps)

    def down(who):
        weights = jnp.concatenate(
            [
                lax.dynamic_slice(
                    full_down, ((((y + k) % NY) * NC + who) * span, 0), (span, ff)
                )
                for k in range(NY)
            ],
            axis=0,
        )
        return lax.dot_general(
            hidden, weights, (((1,), (1,)), ((), ())), preferred_element_type=jnp.float32
        )

    got = swap(down(1 - core).astype(jnp.bfloat16))
    pair = (down(core) + got.astype(jnp.float32)).astype(jnp.bfloat16)
    pairs = [pair[:, k * span : (k + 1) * span] for k in range(NY)]
    ffn_cols = pairs[0].astype(jnp.float32)
    for block in to_owners(pairs):
        ffn_cols = ffn_cols + block.astype(jnp.float32)
    return (mixed_own.astype(jnp.float32) + ffn_cols).astype(jnp.bfloat16)


def solution(mesh):
    grid = Mesh(mesh.devices.reshape(NZ, NX, NY, NC), AXES)
    sp, tp = ("z", "x"), ("y", "core")
    placed = (
        P(sp, tp),
        P(sp, tp),
        P(sp, tp),
        P(tp),
        P(sp),
        P(sp, None),
        P(tp, None),
        P(),
        P(sp, tp),
        P(sp, tp),
        P(None, tp),
        P(sp, tp),
    )
    return jax.shard_map(
        per_device, mesh=grid, in_specs=placed, out_specs=P(sp, tp), check_vma=False
    )
```

```python
import functools

import jax
import jax.numpy as jnp
from jax import lax
from jax.experimental import pallas as pl
from jax.experimental.pallas import tpu as pltpu
from jax.sharding import Mesh
from jax.sharding import PartitionSpec as P

HEAD_DIM = 64
WINDOW = 128
EPS = 1e-06
NEG = -1e30

NZ, NX, NY, NC = 8, 4, 4, 2
AXES = ("z", "x", "y", "core")
MB = 1 << 20


def index_of(z, x, y, c):
    return (((z % NZ) * NX + x % NX) * NY + y % NY) * NC + c


def send_apart(block, dz, dx):
    pairs = [
        (index_of(z, x, y, c), index_of(z + s * dz, x + s * dx, y, c))
        for z in range(NZ)
        for x in range(NX)
        for y in range(NY)
        for c, s in ((0, 1), (1, -1))
    ]
    return lax.ppermute(block, AXES, pairs)


def send_z(block, k):
    return lax.ppermute(block, "z", [(z, (z + k) % NZ) for z in range(NZ)])


def send_x(block, k):
    return lax.ppermute(block, "x", [(x, (x + k) % NX) for x in range(NX)])


def swap(block):
    return lax.ppermute(block, "core", [(0, 1), (1, 0)])


def after(value, *others):
    return lax.optimization_barrier((value,) + others)[0]


def put(block, piece, *at):
    piece = piece.reshape((1,) * (block.ndim - piece.ndim) + piece.shape)
    start = list(at) + [0] * (block.ndim - len(at))
    return lax.dynamic_update_slice(block, piece, start)


def attention_kernel(
    at_ref, sink_ref, q_ref, w_ref, packed_ref, low_ref, high_ref,
    theirs_ref, mine_ref, same_ref,
    att_ref, kx_ref, vx_ref, row_ref, col_ref,
):
    rows = q_ref.shape[0]
    heads = q_ref.shape[1] // HEAD_DIM
    span = theirs_ref.shape[2]
    kx_ref[...] = jnp.zeros_like(kx_ref)
    vx_ref[...] = jnp.zeros_like(vx_ref)
    pieces = (
        (0, WINDOW, low_ref[:HEAD_DIM], low_ref[HEAD_DIM : 2 * HEAD_DIM]),
        (WINDOW, rows, packed_ref[:HEAD_DIM], packed_ref[HEAD_DIM : 2 * HEAD_DIM]),
        (WINDOW + rows, WINDOW, high_ref[:HEAD_DIM], high_ref[HEAD_DIM : 2 * HEAD_DIM]),
    )
    for start, width, keys, vals in pieces:
        vals_t = vals.astype(jnp.float32).T.astype(jnp.bfloat16)
        for h in range(heads):
            kx_ref[h, h * HEAD_DIM : (h + 1) * HEAD_DIM, start : start + width] = keys
            vx_ref[h, start : start + width, h * HEAD_DIM : (h + 1) * HEAD_DIM] = vals_t
    row_ref[:, :WINDOW] = jnp.broadcast_to(
        low_ref[2 * HEAD_DIM :].astype(jnp.float32), (8, WINDOW)
    )
    row_ref[:, WINDOW : WINDOW + rows] = jnp.broadcast_to(
        packed_ref[2 * HEAD_DIM :].astype(jnp.float32), (8, rows)
    )
    row_ref[:, WINDOW + rows :] = jnp.broadcast_to(
        high_ref[2 * HEAD_DIM :].astype(jnp.float32), (8, WINDOW)
    )
    for n in range(rows // WINDOW):
        part = row_ref[:, (n + 1) * WINDOW : (n + 2) * WINDOW]
        col_ref[n * WINDOW : (n + 1) * WINDOW, :] = jnp.broadcast_to(
            part[:1], (WINDOW, WINDOW)
        ).T

    label = col_ref[...]
    at_row = lax.broadcasted_iota(jnp.int32, (rows, WINDOW), 0)
    at_lane = lax.broadcasted_iota(jnp.int32, (rows, WINDOW), 1)
    first, last = row_ref[:1, WINDOW - 1 : WINDOW], row_ref[:1, WINDOW + rows : WINDOW + rows + 1]
    prior = jnp.where(at_row == 0, first, pltpu.roll(label, 1, 0))
    following = jnp.where(at_row == rows - 1, last, pltpu.roll(label, rows - 1, 0))
    other = jnp.where(at_lane == 0, prior, following)
    same_ref[...] = jnp.where(other == label, 1.0, 0.0)

    def step(n, carry):
        base = pl.multiple_of(n * WINDOW, WINDOW)
        here = pl.ds(base, WINDOW)
        window = pl.ds(base, 3 * WINDOW)
        q = q_ref[here, :] * jnp.bfloat16(HEAD_DIM ** (-0.5))
        offsets = (
            lax.broadcasted_iota(jnp.int32, (WINDOW, 3 * WINDOW), 1)
            - WINDOW
            - lax.broadcasted_iota(jnp.int32, (WINDOW, 3 * WINDOW), 0)
        )
        mine = col_ref[here, :1]
        allowed = (jnp.abs(offsets) <= WINDOW) & (row_ref[:1, window] == mine)
        acc = None
        for h in range(heads):
            score = jnp.dot(q, kx_ref[h, :, window], preferred_element_type=jnp.float32)
            score = jnp.where(allowed, score, NEG)
            highest = jnp.maximum(jnp.max(score, axis=1, keepdims=True), sink_ref[h])
            raw = jnp.exp(score - highest)
            total = jnp.sum(raw, axis=1, keepdims=True) + jnp.exp(sink_ref[h] - highest)
            probs = (raw * (1.0 / total)).astype(jnp.bfloat16)
            part = jnp.dot(probs, vx_ref[h, window, :], preferred_element_type=jnp.float32)
            acc = part if acc is None else acc + part
        att_ref[here, :] = acc.astype(jnp.bfloat16)
        return carry

    lax.fori_loop(0, rows // WINDOW, step, 0)
    for k in range(NY):
        cols = pl.ds(pl.multiple_of(at_ref[NY + k] * span, span), span)
        theirs_ref[k] = jnp.dot(
            att_ref[...], w_ref[:, cols], preferred_element_type=jnp.float32
        ).astype(jnp.bfloat16)
        cols = pl.ds(pl.multiple_of(at_ref[k] * span, span), span)
        mine_ref[k] = jnp.dot(
            att_ref[...], w_ref[:, cols], preferred_element_type=jnp.float32
        ).astype(jnp.bfloat16)


def vmem_specs(count):
    return [pl.BlockSpec(memory_space=pltpu.VMEM)] * count


def smem_specs(count):
    return [pl.BlockSpec(memory_space=pltpu.SMEM)] * count


def attention(order, sink, queries, packed, low, high, w_out):
    rows, cols = queries.shape
    span = w_out.shape[1] // (NY * NC)
    reach = rows + 2 * WINDOW
    heads = cols // HEAD_DIM
    return pl.pallas_call(
        attention_kernel,
        out_shape=[
            jax.ShapeDtypeStruct((NY, rows, span), jnp.bfloat16),
            jax.ShapeDtypeStruct((NY, rows, span), jnp.bfloat16),
            jax.ShapeDtypeStruct((rows, WINDOW), jnp.float32),
        ],
        in_specs=smem_specs(2) + vmem_specs(5),
        out_specs=vmem_specs(3),
        scratch_shapes=[
            pltpu.VMEM((rows, cols), jnp.bfloat16),
            pltpu.VMEM((heads, cols, reach), jnp.bfloat16),
            pltpu.VMEM((heads, reach, cols), jnp.bfloat16),
            pltpu.VMEM((8, reach), jnp.float32),
            pltpu.VMEM((rows, WINDOW), jnp.float32),
        ],
        compiler_params=pltpu.CompilerParams(vmem_limit_bytes=12 * MB),
        cost_estimate=pl.CostEstimate(flops=4 * 10**9, bytes_accessed=4 * MB, transcendentals=0),
        name="attention",
    )(order, sink, queries, w_out, packed, low, high)


def pair_kernel(mine_ref, got_ref, s0, s1, s2, s3):
    for k, out in enumerate((s0, s1, s2, s3)):
        out[...] = (
            mine_ref[k].astype(jnp.float32) + got_ref[k].astype(jnp.float32)
        ).astype(jnp.bfloat16)


def pair_sums(mine, got):
    return pl.pallas_call(
        pair_kernel,
        out_shape=[jax.ShapeDtypeStruct(got.shape[1:], jnp.bfloat16)] * NY,
        in_specs=vmem_specs(2),
        out_specs=vmem_specs(NY),
        compiler_params=pltpu.CompilerParams(vmem_limit_bytes=8 * MB),
        cost_estimate=pl.CostEstimate(flops=10**9, bytes_accessed=4 * MB, transcendentals=0),
        name="pair_sums",
    )(mine, got)


def norm_kernel(at_ref, p0, p1, p2, p3, rest_ref, gain_ref, out_ref):
    rows, span = p0.shape
    width = out_ref.shape[1]

    def step(n, carry):
        here = pl.ds(pl.multiple_of(n * 64, 64), 64)
        mine = [ref[here, :].astype(jnp.float32) for ref in (p0, p1, p2, p3)]
        theirs = [rest_ref[k, here, :].astype(jnp.float32) for k in range(NY)]
        square = sum(block * block for block in mine + theirs)
        mean_sq = jnp.sum(square, axis=1, keepdims=True) * (1.0 / width)
        scale = lax.rsqrt(mean_sq + EPS)
        for k, block in enumerate(mine + theirs):
            cols = pl.ds(pl.multiple_of(at_ref[2 * NY + k] * span, span), span)
            out_ref[here, cols] = (block * scale * gain_ref[:, cols]).astype(jnp.bfloat16)
        return carry

    lax.fori_loop(0, rows // 64, step, 0)


def normalised(order, parts, rest, gain):
    rows, _ = parts[0].shape
    return pl.pallas_call(
        norm_kernel,
        out_shape=jax.ShapeDtypeStruct((rows, gain.shape[1]), jnp.bfloat16),
        in_specs=smem_specs(1) + vmem_specs(NY + 2),
        out_specs=pl.BlockSpec(memory_space=pltpu.VMEM),
        compiler_params=pltpu.CompilerParams(vmem_limit_bytes=10 * MB),
        cost_estimate=pl.CostEstimate(flops=2 * 10**9, bytes_accessed=6 * MB, transcendentals=0),
        name="normalise",
    )(order, *parts, rest, gain)


def up_kernel(start, left_ref, w_ref, out_ref):
    width = out_ref.shape[1]

    def step(n, carry):
        here = pl.ds(pl.multiple_of(n * 256, 256), 256)
        out_ref[here, :] = jnp.dot(
            left_ref[here, :], w_ref[:, start : start + width], preferred_element_type=jnp.float32
        ).astype(jnp.bfloat16)
        return carry

    lax.fori_loop(0, left_ref.shape[0] // 256, step, 0)


def up(left, weights, start, width):
    return pl.pallas_call(
        functools.partial(up_kernel, start),
        out_shape=jax.ShapeDtypeStruct((left.shape[0], width), jnp.bfloat16),
        in_specs=vmem_specs(2),
        out_specs=pl.BlockSpec(memory_space=pltpu.VMEM),
        compiler_params=pltpu.CompilerParams(vmem_limit_bytes=14 * MB),
        cost_estimate=pl.CostEstimate(flops=3 * 10**9, bytes_accessed=8 * MB, transcendentals=0),
    )(left, weights)


def hidden_kernel(value_ref, gate_ref, same_ref, before_ref, behind_ref, taps_ref, out_ref):
    rows, ff = out_ref.shape
    tail = gate_ref.shape[1]
    width = value_ref.shape[1]
    chunk = 256
    count = rows // chunk
    row = lax.broadcasted_iota(jnp.int32, (chunk, 128), 0)

    for at in range(0, width, 128):
        cols = slice(at, at + 128)
        if at < tail:
            low, high = before_ref[:, cols], behind_ref[:, cols]
            taps = taps_ref[:, cols].astype(jnp.float32)
        else:
            pad = ((0, 0), (0, at + 128 - ff))
            low, high = jnp.pad(before_ref[:, at:ff], pad), jnp.pad(behind_ref[:, at:ff], pad)
            taps = jnp.pad(taps_ref[:, at:ff].astype(jnp.float32), pad)
        low, high = low.astype(jnp.float32), high.astype(jnp.float32)

        def step(n, above):
            base = pl.multiple_of(n * chunk, chunk)
            here = pl.ds(base, chunk)
            value = value_ref[here, cols].astype(jnp.float32)
            following = pl.ds(pl.multiple_of(jnp.minimum(base + chunk, rows - 16), 16), 16)
            below = value_ref[following, cols].astype(jnp.float32)[:1]
            below = jnp.where(n == count - 1, high, below)
            prior = jnp.where(row == 0, above, pltpu.roll(value, 1, 0))
            after_ = jnp.where(row == chunk - 1, below, pltpu.roll(value, chunk - 1, 0))
            prev_same, next_same = same_ref[here, :1] > 0.5, same_ref[here, 1:2] > 0.5
            conv = (
                taps[0:1] * jnp.where(prev_same, prior, 0.0)
                + taps[1:2] * value
                + taps[2:3] * jnp.where(next_same, after_, 0.0)
            )
            act = conv * lax.logistic(conv)
            if at < tail:
                out_ref[here, cols] = (act * gate_ref[here, cols].astype(jnp.float32)).astype(
                    jnp.bfloat16
                )
            else:
                gate = pltpu.roll(value, 64, 1)
                out_ref[here, at:ff] = (act * gate).astype(jnp.bfloat16)[:, : ff - at]
            return value[chunk - 1 :]

        lax.fori_loop(0, count, step, low)


def hidden_units(value, gate, same, before, behind, taps):
    rows, ff = value.shape[0], taps.shape[1]
    return pl.pallas_call(
        hidden_kernel,
        out_shape=jax.ShapeDtypeStruct((rows, ff), jnp.bfloat16),
        in_specs=vmem_specs(6),
        out_specs=pl.BlockSpec(memory_space=pltpu.VMEM),
        compiler_params=pltpu.CompilerParams(vmem_limit_bytes=8 * MB),
        cost_estimate=pl.CostEstimate(flops=2 * 10**9, bytes_accessed=4 * MB, transcendentals=0),
        name="hidden_units",
    )(value, gate, same, before, behind, taps)


def to_owners(pairs):
    got = []
    for k in range(1, NY):
        got.append(lax.ppermute(pairs[k], "y", [(y, (y + k) % NY) for y in range(NY)]))
    return got


def per_device(
    queries,
    key_rows,
    values,
    sink_logits,
    doc_ids,
    residual,
    w_out,
    norm_gain,
    w_value_up,
    w_gate_up,
    conv_taps,
    w_down_t,
):
    model_width = residual.shape[1]
    span = model_width // (NY * NC)
    ff = w_value_up.shape[1]
    z, x, y, core = (lax.axis_index(axis) for axis in AXES)
    tp = y * NC + core
    order = jnp.stack(
        [((y + k) % NY) * NC + who for who in (core, 1 - core) for k in range(NY)]
        + [((y - k) % NY) * NC + who for who in (core, 1 - core) for k in range(NY)]
    )
    count = NZ * NX
    forward = [(i, i + 1) for i in range(count - 1)]
    backward = [(target, source) for source, target in forward]

    keys_t, vals_t = key_rows.T, values.T
    labels = (doc_ids + 1).astype(jnp.float32)[None, :]
    packed = jnp.concatenate([keys_t, vals_t, labels.astype(jnp.bfloat16)], axis=0)
    low = lax.ppermute(packed[:, -WINDOW:], ("z", "x"), forward)
    high = lax.ppermute(packed[:, :WINDOW], ("z", "x"), backward)

    tail = ff - ff % 128
    first = after(w_value_up, packed)
    share = jnp.concatenate(
        [w_gate_up[:, :tail], first, w_gate_up[:, tail:]], axis=1
    )
    rows_w, width = share.shape
    gathered = []
    for k in range(1, NX):
        gathered.append(send_x(share, k))

    def ring_step(plus, minus):
        plus = send_z(plus, 1)
        minus = send_z(minus, -1)
        return plus, minus

    def keep(full, plus, minus, k):
        return put(put(full, plus, (z - k) % NZ), minus, (z + k) % NZ)

    theirs, mine, same = attention(order, sink_logits, queries, packed, low, high, w_out)
    got = swap(theirs)

    gathered = lax.optimization_barrier((*gathered, theirs))[:-1]
    up_rows = put(jnp.zeros((NX, rows_w, width), share.dtype), share, x)
    for k, piece in enumerate(gathered):
        up_rows = put(up_rows, piece, (x - k - 1) % NX)
    up_rows = up_rows.reshape(NX * rows_w, width)
    plus1, minus1 = ring_step(up_rows, up_rows)

    pairs = pair_sums(mine, got)
    sent = to_owners(pairs)

    down1 = after(w_down_t, pairs[0])
    near = ring_step(down1, down1)
    far_plus = send_z(down1, 2)
    far_minus = send_z(down1, -2)

    plus2, minus2 = ring_step(plus1, minus1)
    own_res = lax.dynamic_slice_in_dim(residual, tp * span, span, 1)
    summed = pairs[0].astype(jnp.float32)
    for block in sent:
        summed = summed + block.astype(jnp.float32)
    mixed_own = (own_res.astype(jnp.float32) + summed).astype(jnp.bfloat16)

    far_plus, far_minus = lax.optimization_barrier((far_plus, far_minus, mixed_own))[:2]
    third = ring_step(far_plus, far_minus)
    last_down = send_apart(jnp.where(core == 0, far_plus, far_minus), 2, 0)

    came = to_owners([mixed_own] * NY)
    came = lax.optimization_barrier((*came, plus2, minus2))[: NY - 1]
    parts = [mixed_own, *came]
    plus3, minus3 = ring_step(plus2, minus2)
    full = put(jnp.zeros((NZ,) + up_rows.shape, share.dtype), after(up_rows, mixed_own), z)
    full = keep(full, plus1, minus1, 1)
    whole = jnp.zeros((NZ,) + w_down_t.shape, w_down_t.dtype)
    whole = put(whole, after(w_down_t, mixed_own, plus2, minus2), z)
    whole = keep(whole, *near, 1)
    whole = keep(whole, far_plus, far_minus, 2)
    whole = keep(whole, *third, 3)
    whole = put(whole, last_down, (z + NZ // 2) % NZ)
    whole_plus = send_x(whole, 1)
    whole_minus = send_x(whole, -1)

    stacked = jnp.stack(parts)
    rest = swap(stacked)
    last = send_apart(jnp.where(core == 0, plus3, minus3), 1, 0)
    normed = normalised(order, parts, rest, norm_gain[None])
    full = keep(after(full, normed), plus2, minus2, 2)
    full = keep(full, plus3, minus3, 3)

    full_down = jnp.zeros((NZ, NX, rows_w, ff), w_down_t.dtype)
    full_down = put(full_down, after(whole, normed)[:, None], 0, x)
    full, full_down, whole_plus, whole_minus = lax.optimization_barrier(
        (full, full_down, whole_plus, whole_minus)
    )
    full = put(full, last, (z + NZ // 2) % NZ).reshape(model_width, width)
    whole_far = send_apart(jnp.where(core == 0, whole_plus, whole_minus), 0, 1)
    full_down = put(full_down, whole_plus[:, None], 0, (x - 1) % NX)
    full_down = put(full_down, whole_minus[:, None], 0, (x + 1) % NX)
    normed = after(normed, full_down)
    full_down = put(full_down, whole_far[:, None], 0, (x + 2) % NX).reshape(model_width, ff)

    up_value = up(normed, full, tail, width - tail)
    before = lax.ppermute(up_value[-1:, :ff], ("z", "x"), forward)
    behind = lax.ppermute(up_value[:1, :ff], ("z", "x"), backward)
    up_gate = up(normed, full, 0, tail)
    hidden = hidden_units(up_value, up_gate, same, before, behind, conv_taps)

    def down(who):
        weights = jnp.concatenate(
            [
                lax.dynamic_slice(
                    full_down, ((((y + k) % NY) * NC + who) * span, 0), (span, ff)
                )
                for k in range(NY)
            ],
            axis=0,
        )
        return lax.dot_general(
            hidden, weights, (((1,), (1,)), ((), ())), preferred_element_type=jnp.float32
        )

    theirs = down(1 - core).astype(jnp.bfloat16)
    got = swap(theirs)
    mine = after(down(core).astype(jnp.bfloat16), theirs)
    pair = (mine.astype(jnp.float32) + got.astype(jnp.float32)).astype(jnp.bfloat16)
    pairs = [pair[:, k * span : (k + 1) * span] for k in range(NY)]
    ffn_cols = pairs[0].astype(jnp.float32)
    for block in to_owners(pairs):
        ffn_cols = ffn_cols + block.astype(jnp.float32)
    return (mixed_own.astype(jnp.float32) + ffn_cols).astype(jnp.bfloat16)


def solution(mesh):
    grid = Mesh(mesh.devices.reshape(NZ, NX, NY, NC), AXES)
    sp, tp = ("z", "x"), ("y", "core")
    placed = (
        P(sp, tp),
        P(sp, tp),
        P(sp, tp),
        P(tp),
        P(sp),
        P(sp, None),
        P(tp, None),
        P(),
        P(sp, tp),
        P(sp, tp),
        P(None, tp),
        P(sp, tp),
    )
    return jax.shard_map(
        per_device, mesh=grid, in_specs=placed, out_specs=P(sp, tp), check_vma=False
    )
```

```python
import functools

import jax
import jax.numpy as jnp
from jax import lax
from jax.experimental import pallas as pl
from jax.experimental.pallas import tpu as pltpu
from jax.sharding import Mesh
from jax.sharding import PartitionSpec as P

HEAD_DIM = 64
WINDOW = 128
EPS = 1e-06
NEG = -1e30

NZ, NX, NY, NC = 8, 4, 4, 2
AXES = ("z", "x", "y", "core")
MB = 1 << 20


def index_of(z, x, y, c):
    return (((z % NZ) * NX + x % NX) * NY + y % NY) * NC + c


def send_apart(block, dz, dx):
    pairs = [
        (index_of(z, x, y, c), index_of(z + s * dz, x + s * dx, y, c))
        for z in range(NZ)
        for x in range(NX)
        for y in range(NY)
        for c, s in ((0, 1), (1, -1))
    ]
    return lax.ppermute(block, AXES, pairs)


def send_z(block, k):
    return lax.ppermute(block, "z", [(z, (z + k) % NZ) for z in range(NZ)])


def send_x(block, k):
    return lax.ppermute(block, "x", [(x, (x + k) % NX) for x in range(NX)])


def swap(block):
    return lax.ppermute(block, "core", [(0, 1), (1, 0)])


def after(value, *others):
    return lax.optimization_barrier((value,) + others)[0]


def put(block, piece, *at):
    piece = piece.reshape((1,) * (block.ndim - piece.ndim) + piece.shape)
    start = list(at) + [0] * (block.ndim - len(at))
    return lax.dynamic_update_slice(block, piece, start)


def attention_kernel(
    at_ref, sink_ref, q_ref, w_ref, packed_ref, low_ref, high_ref,
    theirs_ref, mine_ref, same_ref,
    att_ref, kx_ref, vx_ref, row_ref, col_ref,
):
    rows = q_ref.shape[0]
    heads = q_ref.shape[1] // HEAD_DIM
    span = theirs_ref.shape[2]
    kx_ref[...] = jnp.zeros_like(kx_ref)
    vx_ref[...] = jnp.zeros_like(vx_ref)
    pieces = (
        (0, WINDOW, low_ref[:HEAD_DIM], low_ref[HEAD_DIM : 2 * HEAD_DIM]),
        (WINDOW, rows, packed_ref[:HEAD_DIM], packed_ref[HEAD_DIM : 2 * HEAD_DIM]),
        (WINDOW + rows, WINDOW, high_ref[:HEAD_DIM], high_ref[HEAD_DIM : 2 * HEAD_DIM]),
    )
    for start, width, keys, vals in pieces:
        vals_t = vals.astype(jnp.float32).T.astype(jnp.bfloat16)
        for h in range(heads):
            kx_ref[h, h * HEAD_DIM : (h + 1) * HEAD_DIM, start : start + width] = keys
            vx_ref[h, start : start + width, h * HEAD_DIM : (h + 1) * HEAD_DIM] = vals_t
    row_ref[:, :WINDOW] = jnp.broadcast_to(
        low_ref[2 * HEAD_DIM :].astype(jnp.float32), (8, WINDOW)
    )
    row_ref[:, WINDOW : WINDOW + rows] = jnp.broadcast_to(
        packed_ref[2 * HEAD_DIM :].astype(jnp.float32), (8, rows)
    )
    row_ref[:, WINDOW + rows :] = jnp.broadcast_to(
        high_ref[2 * HEAD_DIM :].astype(jnp.float32), (8, WINDOW)
    )
    for n in range(rows // WINDOW):
        part = row_ref[:, (n + 1) * WINDOW : (n + 2) * WINDOW]
        col_ref[n * WINDOW : (n + 1) * WINDOW, :] = jnp.broadcast_to(
            part[:1], (WINDOW, WINDOW)
        ).T

    label = col_ref[...]
    at_row = lax.broadcasted_iota(jnp.int32, (rows, WINDOW), 0)
    at_lane = lax.broadcasted_iota(jnp.int32, (rows, WINDOW), 1)
    first, last = row_ref[:1, WINDOW - 1 : WINDOW], row_ref[:1, WINDOW + rows : WINDOW + rows + 1]
    prior = jnp.where(at_row == 0, first, pltpu.roll(label, 1, 0))
    following = jnp.where(at_row == rows - 1, last, pltpu.roll(label, rows - 1, 0))
    other = jnp.where(at_lane == 0, prior, following)
    same_ref[...] = jnp.where(other == label, 1.0, 0.0)

    def step(n, carry):
        base = pl.multiple_of(n * WINDOW, WINDOW)
        here = pl.ds(base, WINDOW)
        window = pl.ds(base, 3 * WINDOW)
        q = q_ref[here, :] * jnp.bfloat16(HEAD_DIM ** (-0.5))
        offsets = (
            lax.broadcasted_iota(jnp.int32, (WINDOW, 3 * WINDOW), 1)
            - WINDOW
            - lax.broadcasted_iota(jnp.int32, (WINDOW, 3 * WINDOW), 0)
        )
        mine = col_ref[here, :1]
        allowed = (jnp.abs(offsets) <= WINDOW) & (row_ref[:1, window] == mine)
        acc = None
        for h in range(heads):
            score = jnp.dot(q, kx_ref[h, :, window], preferred_element_type=jnp.float32)
            score = jnp.where(allowed, score, NEG)
            highest = jnp.maximum(jnp.max(score, axis=1, keepdims=True), sink_ref[h])
            raw = jnp.exp(score - highest)
            total = jnp.sum(raw, axis=1, keepdims=True) + jnp.exp(sink_ref[h] - highest)
            probs = (raw * (1.0 / total)).astype(jnp.bfloat16)
            part = jnp.dot(probs, vx_ref[h, window, :], preferred_element_type=jnp.float32)
            acc = part if acc is None else acc + part
        att_ref[here, :] = acc.astype(jnp.bfloat16)
        return carry

    lax.fori_loop(0, rows // WINDOW, step, 0)
    for k in range(NY):
        cols = pl.ds(pl.multiple_of(at_ref[NY + k] * span, span), span)
        theirs_ref[k] = jnp.dot(
            att_ref[...], w_ref[:, cols], preferred_element_type=jnp.float32
        ).astype(jnp.bfloat16)
        cols = pl.ds(pl.multiple_of(at_ref[k] * span, span), span)
        mine_ref[k] = jnp.dot(
            att_ref[...], w_ref[:, cols], preferred_element_type=jnp.float32
        ).astype(jnp.bfloat16)


def vmem_specs(count):
    return [pl.BlockSpec(memory_space=pltpu.VMEM)] * count


def smem_specs(count):
    return [pl.BlockSpec(memory_space=pltpu.SMEM)] * count


def attention(order, sink, queries, packed, low, high, w_out):
    rows, cols = queries.shape
    span = w_out.shape[1] // (NY * NC)
    reach = rows + 2 * WINDOW
    heads = cols // HEAD_DIM
    return pl.pallas_call(
        attention_kernel,
        out_shape=[
            jax.ShapeDtypeStruct((NY, rows, span), jnp.bfloat16),
            jax.ShapeDtypeStruct((NY, rows, span), jnp.bfloat16),
            jax.ShapeDtypeStruct((rows, WINDOW), jnp.float32),
        ],
        in_specs=smem_specs(2) + vmem_specs(5),
        out_specs=vmem_specs(3),
        scratch_shapes=[
            pltpu.VMEM((rows, cols), jnp.bfloat16),
            pltpu.VMEM((heads, cols, reach), jnp.bfloat16),
            pltpu.VMEM((heads, reach, cols), jnp.bfloat16),
            pltpu.VMEM((8, reach), jnp.float32),
            pltpu.VMEM((rows, WINDOW), jnp.float32),
        ],
        compiler_params=pltpu.CompilerParams(vmem_limit_bytes=12 * MB),
        cost_estimate=pl.CostEstimate(flops=4 * 10**9, bytes_accessed=4 * MB, transcendentals=0),
        name="attention",
    )(order, sink, queries, w_out, packed, low, high)


def pair_kernel(mine_ref, got_ref, s0, s1, s2, s3):
    for k, out in enumerate((s0, s1, s2, s3)):
        out[...] = (
            mine_ref[k].astype(jnp.float32) + got_ref[k].astype(jnp.float32)
        ).astype(jnp.bfloat16)


def pair_sums(mine, got):
    return pl.pallas_call(
        pair_kernel,
        out_shape=[jax.ShapeDtypeStruct(got.shape[1:], jnp.bfloat16)] * NY,
        in_specs=vmem_specs(2),
        out_specs=vmem_specs(NY),
        compiler_params=pltpu.CompilerParams(vmem_limit_bytes=8 * MB),
        cost_estimate=pl.CostEstimate(flops=10**9, bytes_accessed=4 * MB, transcendentals=0),
        name="pair_sums",
    )(mine, got)


def norm_kernel(at_ref, p0, p1, p2, p3, rest_ref, gain_ref, out_ref):
    rows, span = p0.shape
    width = out_ref.shape[1]

    def step(n, carry):
        here = pl.ds(pl.multiple_of(n * 64, 64), 64)
        mine = [ref[here, :].astype(jnp.float32) for ref in (p0, p1, p2, p3)]
        theirs = [rest_ref[k, here, :].astype(jnp.float32) for k in range(NY)]
        square = sum(block * block for block in mine + theirs)
        mean_sq = jnp.sum(square, axis=1, keepdims=True) * (1.0 / width)
        scale = lax.rsqrt(mean_sq + EPS)
        for k, block in enumerate(mine + theirs):
            cols = pl.ds(pl.multiple_of(at_ref[2 * NY + k] * span, span), span)
            out_ref[here, cols] = (block * scale * gain_ref[:, cols]).astype(jnp.bfloat16)
        return carry

    lax.fori_loop(0, rows // 64, step, 0)


def normalised(order, parts, rest, gain):
    rows, _ = parts[0].shape
    return pl.pallas_call(
        norm_kernel,
        out_shape=jax.ShapeDtypeStruct((rows, gain.shape[1]), jnp.bfloat16),
        in_specs=smem_specs(1) + vmem_specs(NY + 2),
        out_specs=pl.BlockSpec(memory_space=pltpu.VMEM),
        compiler_params=pltpu.CompilerParams(vmem_limit_bytes=10 * MB),
        cost_estimate=pl.CostEstimate(flops=2 * 10**9, bytes_accessed=6 * MB, transcendentals=0),
        name="normalise",
    )(order, *parts, rest, gain)


def up_kernel(start, left_ref, w_ref, out_ref):
    width = out_ref.shape[1]

    def step(n, carry):
        here = pl.ds(pl.multiple_of(n * 256, 256), 256)
        out_ref[here, :] = jnp.dot(
            left_ref[here, :], w_ref[:, start : start + width], preferred_element_type=jnp.float32
        ).astype(jnp.bfloat16)
        return carry

    lax.fori_loop(0, left_ref.shape[0] // 256, step, 0)


def up(left, weights, start, width):
    return pl.pallas_call(
        functools.partial(up_kernel, start),
        out_shape=jax.ShapeDtypeStruct((left.shape[0], width), jnp.bfloat16),
        in_specs=vmem_specs(2),
        out_specs=pl.BlockSpec(memory_space=pltpu.VMEM),
        compiler_params=pltpu.CompilerParams(vmem_limit_bytes=14 * MB),
        cost_estimate=pl.CostEstimate(flops=3 * 10**9, bytes_accessed=8 * MB, transcendentals=0),
    )(left, weights)


def hidden_kernel(value_ref, gate_ref, same_ref, before_ref, behind_ref, taps_ref, out_ref):
    rows, ff = out_ref.shape
    tail = gate_ref.shape[1]
    width = value_ref.shape[1]
    chunk = 256
    count = rows // chunk
    row = lax.broadcasted_iota(jnp.int32, (chunk, 128), 0)

    for at in range(0, width, 128):
        cols = slice(at, at + 128)
        if at < tail:
            low, high = before_ref[:, cols], behind_ref[:, cols]
            taps = taps_ref[:, cols].astype(jnp.float32)
        else:
            pad = ((0, 0), (0, at + 128 - ff))
            low, high = jnp.pad(before_ref[:, at:ff], pad), jnp.pad(behind_ref[:, at:ff], pad)
            taps = jnp.pad(taps_ref[:, at:ff].astype(jnp.float32), pad)
        low, high = low.astype(jnp.float32), high.astype(jnp.float32)

        def step(n, above):
            base = pl.multiple_of(n * chunk, chunk)
            here = pl.ds(base, chunk)
            value = value_ref[here, cols].astype(jnp.float32)
            following = pl.ds(pl.multiple_of(jnp.minimum(base + chunk, rows - 16), 16), 16)
            below = value_ref[following, cols].astype(jnp.float32)[:1]
            below = jnp.where(n == count - 1, high, below)
            prior = jnp.where(row == 0, above, pltpu.roll(value, 1, 0))
            after_ = jnp.where(row == chunk - 1, below, pltpu.roll(value, chunk - 1, 0))
            prev_same, next_same = same_ref[here, :1] > 0.5, same_ref[here, 1:2] > 0.5
            conv = (
                taps[0:1] * jnp.where(prev_same, prior, 0.0)
                + taps[1:2] * value
                + taps[2:3] * jnp.where(next_same, after_, 0.0)
            )
            act = conv * lax.logistic(conv)
            if at < tail:
                out_ref[here, cols] = (act * gate_ref[here, cols].astype(jnp.float32)).astype(
                    jnp.bfloat16
                )
            else:
                gate = pltpu.roll(value, 64, 1)
                out_ref[here, at:ff] = (act * gate).astype(jnp.bfloat16)[:, : ff - at]
            return value[chunk - 1 :]

        lax.fori_loop(0, count, step, low)


def hidden_units(value, gate, same, before, behind, taps):
    rows, ff = value.shape[0], taps.shape[1]
    return pl.pallas_call(
        hidden_kernel,
        out_shape=jax.ShapeDtypeStruct((rows, ff), jnp.bfloat16),
        in_specs=vmem_specs(6),
        out_specs=pl.BlockSpec(memory_space=pltpu.VMEM),
        compiler_params=pltpu.CompilerParams(vmem_limit_bytes=8 * MB),
        cost_estimate=pl.CostEstimate(flops=2 * 10**9, bytes_accessed=4 * MB, transcendentals=0),
        name="hidden_units",
    )(value, gate, same, before, behind, taps)


def to_owners(pairs):
    got = []
    for k in range(1, NY):
        got.append(lax.ppermute(pairs[k], "y", [(y, (y + k) % NY) for y in range(NY)]))
    return got


def per_device(
    queries,
    key_rows,
    values,
    sink_logits,
    doc_ids,
    residual,
    w_out,
    norm_gain,
    w_value_up,
    w_gate_up,
    conv_taps,
    w_down_t,
):
    model_width = residual.shape[1]
    span = model_width // (NY * NC)
    ff = w_value_up.shape[1]
    z, x, y, core = (lax.axis_index(axis) for axis in AXES)
    tp = y * NC + core
    order = jnp.stack(
        [((y + k) % NY) * NC + who for who in (core, 1 - core) for k in range(NY)]
        + [((y - k) % NY) * NC + who for who in (core, 1 - core) for k in range(NY)]
    )
    count = NZ * NX
    forward = [(i, i + 1) for i in range(count - 1)]
    backward = [(target, source) for source, target in forward]

    keys_t, vals_t = key_rows.T, values.T
    labels = (doc_ids + 1).astype(jnp.float32)[None, :]
    packed = jnp.concatenate([keys_t, vals_t, labels.astype(jnp.bfloat16)], axis=0)
    low = lax.ppermute(packed[:, -WINDOW:], ("z", "x"), forward)
    high = lax.ppermute(packed[:, :WINDOW], ("z", "x"), backward)

    tail = ff - ff % 128
    first = after(w_value_up, packed)
    share = jnp.concatenate(
        [w_gate_up[:, :tail], first, w_gate_up[:, tail:]], axis=1
    )
    rows_w, width = share.shape
    gathered = []
    for k in range(1, NX):
        gathered.append(send_x(share, k))

    def ring_step(plus, minus):
        plus = send_z(plus, 1)
        minus = send_z(minus, -1)
        return plus, minus

    def keep(full, plus, minus, k):
        return put(put(full, plus, (z - k) % NZ), minus, (z + k) % NZ)

    down1 = after(w_down_t, share)
    near = ring_step(down1, down1)
    far_plus = send_z(down1, 2)
    far_minus = send_z(down1, -2)

    up_rows = put(jnp.zeros((NX, rows_w, width), share.dtype), share, x)
    for k, piece in enumerate(gathered):
        up_rows = put(up_rows, piece, (x - k - 1) % NX)
    up_rows = up_rows.reshape(NX * rows_w, width)
    plus1, minus1 = ring_step(up_rows, up_rows)

    theirs, mine, same = attention(order, sink_logits, queries, packed, low, high, w_out)
    got = swap(theirs)

    pairs = pair_sums(mine, got)
    sent = to_owners(pairs)

    plus2, minus2 = ring_step(plus1, minus1)
    own_res = lax.dynamic_slice_in_dim(residual, tp * span, span, 1)
    summed = pairs[0].astype(jnp.float32)
    for block in sent:
        summed = summed + block.astype(jnp.float32)
    mixed_own = (own_res.astype(jnp.float32) + summed).astype(jnp.bfloat16)

    far_plus, far_minus = lax.optimization_barrier((far_plus, far_minus, pairs[0]))[:2]
    third = ring_step(far_plus, far_minus)
    last_down = send_apart(jnp.where(core == 0, far_plus, far_minus), 2, 0)

    came = to_owners([mixed_own] * NY)
    came = lax.optimization_barrier((*came, plus2, minus2))[: NY - 1]
    parts = [mixed_own, *came]
    plus3, minus3 = ring_step(plus2, minus2)
    full = put(jnp.zeros((NZ,) + up_rows.shape, share.dtype), after(up_rows, mixed_own), z)
    full = keep(full, plus1, minus1, 1)
    whole = jnp.zeros((NZ,) + w_down_t.shape, w_down_t.dtype)
    whole = put(whole, after(w_down_t, mixed_own, plus2, minus2), z)
    whole = keep(whole, *near, 1)
    whole = keep(whole, far_plus, far_minus, 2)
    whole = keep(whole, *third, 3)
    whole = put(whole, last_down, (z + NZ // 2) % NZ)
    whole_plus = send_x(whole, 1)
    whole_minus = send_x(whole, -1)

    stacked = jnp.stack(parts)
    rest = swap(stacked)
    last = send_apart(jnp.where(core == 0, plus3, minus3), 1, 0)
    normed = normalised(order, parts, rest, norm_gain[None])
    full = keep(after(full, normed), plus2, minus2, 2)
    full = keep(full, plus3, minus3, 3)

    full_down = jnp.zeros((NZ, NX, rows_w, ff), w_down_t.dtype)
    full_down = put(full_down, after(whole, normed)[:, None], 0, x)
    full, full_down, whole_plus, whole_minus = lax.optimization_barrier(
        (full, full_down, whole_plus, whole_minus)
    )
    full = put(full, last, (z + NZ // 2) % NZ).reshape(model_width, width)
    whole_far = send_apart(jnp.where(core == 0, whole_plus, whole_minus), 0, 1)
    full_down = put(full_down, whole_plus[:, None], 0, (x - 1) % NX)
    full_down = put(full_down, whole_minus[:, None], 0, (x + 1) % NX)
    normed = after(normed, full_down)
    full_down = put(full_down, whole_far[:, None], 0, (x + 2) % NX).reshape(model_width, ff)

    up_value = up(normed, full, tail, width - tail)
    before = lax.ppermute(up_value[-1:, :ff], ("z", "x"), forward)
    behind = lax.ppermute(up_value[:1, :ff], ("z", "x"), backward)
    up_gate = up(normed, full, 0, tail)
    hidden = hidden_units(up_value, up_gate, same, before, behind, conv_taps)

    def down(who):
        weights = jnp.concatenate(
            [
                lax.dynamic_slice(
                    full_down, ((((y + k) % NY) * NC + who) * span, 0), (span, ff)
                )
                for k in range(NY)
            ],
            axis=0,
        )
        return lax.dot_general(
            hidden, weights, (((1,), (1,)), ((), ())), preferred_element_type=jnp.float32
        )

    theirs = down(1 - core).astype(jnp.bfloat16)
    got = swap(theirs)
    mine = after(down(core).astype(jnp.bfloat16), theirs)
    pair = (mine.astype(jnp.float32) + got.astype(jnp.float32)).astype(jnp.bfloat16)
    pairs = [pair[:, k * span : (k + 1) * span] for k in range(NY)]
    ffn_cols = pairs[0].astype(jnp.float32)
    for block in to_owners(pairs):
        ffn_cols = ffn_cols + block.astype(jnp.float32)
    return (mixed_own.astype(jnp.float32) + ffn_cols).astype(jnp.bfloat16)


def solution(mesh):
    grid = Mesh(mesh.devices.reshape(NZ, NX, NY, NC), AXES)
    sp, tp = ("z", "x"), ("y", "core")
    placed = (
        P(sp, tp),
        P(sp, tp),
        P(sp, tp),
        P(tp),
        P(sp),
        P(sp, None),
        P(tp, None),
        P(),
        P(sp, tp),
        P(sp, tp),
        P(None, tp),
        P(sp, tp),
    )
    return jax.shard_map(
        per_device, mesh=grid, in_specs=placed, out_specs=P(sp, tp), check_vma=False
    )
```
